256 devices in a mesh: sp: 32 (over z, x), tp: 8 (over y, core).
Axes of the slice: x: 4, y: 4, z: 8, core: 2. Of those that a mesh axis runs over, the one named last changes fastest.
Arguments:
- tokens: bfloat16 [16384, 2048], P(('sp', 'tp')), may hold values from -64 to 64
- query_weight: bfloat16 [2048, 2048], P(None, 'tp'), may hold values from -0.125 to 0.125
- key_weight: bfloat16 [2048, 2048], P(None, 'tp'), may hold values from -0.125 to 0.125
- value_weight: bfloat16 [2048, 2048], P(None, 'tp'), may hold values from -0.125 to 0.125
- gate_weight: bfloat16 [2048, 2048], P(None, 'tp'), may hold values from -0.125 to 0.125
- forget_weight: bfloat16 [2048, 16], replicated, may hold values from -0.125 to 0.125
- forget_bias: float32 [16], replicated, as said below
- out_weight: bfloat16 [2048, 2048], replicated, may hold values from -0.125 to 0.125
Outputs:
- mixed: bfloat16 [16384, 2048], P(('sp', 'tp'))
The draws below stay inside these ranges and needn't reach their ends.
Inputs may be any that keep to these rules, and one draw needn't show every extreme that they name: `forget_bias`: every head's forget bias is at least 4.
All inputs are finite; a program needn't handle non-finite values.
Results may differ from the reference program's by a relative error of at most 0.015.
The reference program's roundings to bfloat16 on the way (of `queries`, `keys`, `values` and `attended`) count: a program that leaves them out, or rounds other values in their place, can miss the bound.
Values may be sent and summed in bfloat16 or wider, within the bound.
A program may use at most 128 MiB of HBM per device.

```python
import math
import jax
import jax.numpy as jnp
from jax import lax

D = 2048
HEADS = 16
HEAD_DIM = 128
TOK_DEV = 512
SEQ = 16384


def draw_tokens(key, part):
    keys = jax.random.split(jax.random.fold_in(key, 11), 5)
    span = max(TOK_DEV // 4, 1)
    blocks = SEQ // span
    base = jnp.clip(jax.random.normal(keys[0], (SEQ, D), jnp.float32), -4.0, 4.0)
    shifts = 0.7 * jnp.clip(jax.random.normal(keys[1], (blocks, D), jnp.float32), -2.0, 2.0)
    scales = jnp.exp(jax.random.uniform(keys[2], (blocks, 1), jnp.float32, jnp.log(0.5), jnp.log(2.0)))
    field = (base.reshape(blocks, span, D) + shifts[:, None, :]) * scales[:, None, :]
    field = field.reshape(SEQ, D)
    return jnp.clip(field, -64.0, 64.0).astype(jnp.bfloat16)


def draw_forget_bias(key, part):
    keys = jax.random.split(jax.random.fold_in(key, 23), 2)
    order = jax.random.permutation(keys[0], HEADS)
    fast_count = HEADS // 2
    fast = (order < fast_count).astype(jnp.float32)
    spread = jax.random.uniform(keys[1], (HEADS,), jnp.float32)
    slow_bias = jnp.log(jnp.float32(SEQ)) + 1.0 + spread
    fast_bias = 4.0 + 1.5 * spread
    return fast * fast_bias + (1.0 - fast) * slow_bias


def shard_levels(key, extent, shards, smallest, top_value):
    factor_of = 1.0
    for axis_at, shards_of in shards:
        steps = jax.random.uniform(jax.random.fold_in(jax.random.fold_in(key, 6), axis_at), (shards_of,), jnp.float32, smallest / len(shards), top_value / len(shards))
        factor_of = factor_of * jnp.repeat(jnp.exp(steps), extent[axis_at] // shards_of).reshape((-1,) + (1,) * (len(extent) - 1 - axis_at))
    return factor_of


def noise(stream_key, dims, width, bound, pieces=(), held_as=jnp.bfloat16):
    factor_of = shard_levels(stream_key, dims, pieces, -0.22, 0.18) if pieces else 1.0
    drawn = jax.random.normal(stream_key, dims, jnp.float32) * width * factor_of
    return jnp.minimum(jnp.maximum(drawn, -bound), bound).astype(held_as)


def setup_inputs(seed: int = 0) -> dict:
    streams_of = jax.random.split(jax.random.key(seed), 9)
    tokens = draw_tokens(jax.random.fold_in(streams_of[8], 71), 0)
    query_weight = noise(streams_of[1], (D, D), D ** -0.5, 0.125, ((1, 8),))
    key_weight = noise(streams_of[2], (D, D), D ** -0.5, 0.125, ((1, 8),))
    value_weight = noise(streams_of[3], (D, D), D ** -0.5, 0.125, ((1, 8),))
    gate_weight = noise(streams_of[4], (D, D), D ** -0.5, 0.125, ((1, 8),))
    forget_weight = noise(streams_of[5], (D, HEADS), D ** -0.5, 0.125)
    forget_bias = draw_forget_bias(jax.random.fold_in(streams_of[8], 71), 0)
    out_weight = noise(streams_of[7], (D, D), D ** -0.5, 0.125)
    return {"tokens": tokens, "query_weight": query_weight, "key_weight": key_weight, "value_weight": value_weight, "gate_weight": gate_weight, "forget_weight": forget_weight, "forget_bias": forget_bias, "out_weight": out_weight}


def reference(tokens, query_weight, key_weight, value_weight, gate_weight, forget_weight, forget_bias, out_weight):
    scale = HEAD_DIM ** -0.5
    queries = (jnp.dot(tokens, query_weight, preferred_element_type=jnp.float32) * scale).astype(jnp.bfloat16)
    keys = jnp.dot(tokens, key_weight, preferred_element_type=jnp.float32).astype(jnp.bfloat16)
    values = jnp.dot(tokens, value_weight, preferred_element_type=jnp.float32).astype(jnp.bfloat16)
    gate = jax.nn.sigmoid(jnp.dot(tokens, gate_weight, preferred_element_type=jnp.float32))
    forget_log = jax.nn.log_sigmoid(jnp.dot(tokens, forget_weight, preferred_element_type=jnp.float32) + forget_bias)
    cumul = jnp.cumsum(forget_log.T, axis=1)
    span = math.gcd(SEQ, 512)
    blocks = SEQ // span
    positions = jnp.arange(SEQ, dtype=jnp.int32)

    def one_head(args):
        head_q, head_k, head_v, head_c = args
        query_blocks = head_q.reshape(blocks, span, HEAD_DIM)
        cum_blocks = head_c.reshape(blocks, span)
        pos_blocks = positions.reshape(blocks, span)

        def one_block(inner):
            block_q, block_c, block_p = inner
            scores = jnp.dot(block_q, head_k.T, preferred_element_type=jnp.float32)
            scores = scores + block_c[:, None] - head_c[None, :]
            scores = jnp.where(positions[None, :] <= block_p[:, None], scores, -jnp.inf)
            top = jnp.max(scores, axis=1, keepdims=True)
            weights = jnp.exp(scores - top)
            denom = jnp.sum(weights, axis=1, keepdims=True)
            return jnp.dot(weights.astype(jnp.bfloat16), head_v, preferred_element_type=jnp.float32) / denom

        return lax.map(one_block, (query_blocks, cum_blocks, pos_blocks)).reshape(SEQ, HEAD_DIM)

    split_q = queries.reshape(SEQ, HEADS, HEAD_DIM).transpose(1, 0, 2)
    split_k = keys.reshape(SEQ, HEADS, HEAD_DIM).transpose(1, 0, 2)
    split_v = values.reshape(SEQ, HEADS, HEAD_DIM).transpose(1, 0, 2)
    heads_out = lax.map(one_head, (split_q, split_k, split_v, cumul))
    heads_out = heads_out.transpose(1, 0, 2).reshape(SEQ, D)
    attended = (heads_out * gate).astype(jnp.bfloat16)
    return jnp.dot(attended, out_weight, preferred_element_type=jnp.float32).astype(jnp.bfloat16)
```

```python
import jax
import jax.numpy as jnp
from jax import lax
from jax.experimental import pallas as pl
from jax.experimental.pallas import tpu as pltpu
from jax.sharding import PartitionSpec as P

NZ, NX, NY = 8, 4, 4
HD = 128
WIDTH = 256
D = 2048
SUB = 128
ROW = 64
DELTA = (0, 1, 3, 2)
MESH = pl.DeviceIdType.MESH
NT = (((1,), (1,)), ((), ()))
F32, BF16 = jnp.float32, jnp.bfloat16


def rcopy(src, dst, send, recv, sp, tp):
    return pltpu.make_async_remote_copy(
        src_ref=src,
        dst_ref=dst,
        send_sem=send,
        recv_sem=recv,
        device_id=(sp, tp),
        device_id_type=MESH,
    )


def kernel(
    tok_hbm, wq_hbm, wk_hbm, wv_hbm, wg_hbm, fw_ref, fb_ref, wo_hbm, out_ref,
    tok, wq, wk, wv, wg, wo, kvs, qs, gbuf, ggot, lg, lcs, lcbuf, cu, kv, q, acc, mx, ln, ob, obuf, att,
    loc_s, ty_s, ty_r, tr_s, tr_r, tp_s, tp_r,
    xk_s, xk_r, xq_s, xq_r, g_s, g_r, l_s, l_r, o_s, o_r,
    zs, zr, ps, pr, po_s, po_r,
):
    sp = lax.axis_index("sp")
    tp = lax.axis_index("tp")
    z, x = sp // NX, sp % NX
    y, c = tp // 2, tp % 2
    other = y * 2 + (1 - c)
    up = ((z + 1) % NZ) * NX + x
    down = ((z + NZ - 1) % NZ) * NX + x
    ynext = ((y + 1) % NY) * 2 + c
    yprev = ((y + NY - 1) % NY) * 2 + c
    mine = pl.ds(pl.multiple_of(c * ROW, ROW), ROW)

    tok_cp = pltpu.make_async_copy(tok_hbm, tok.at[0, mine], loc_s.at[0])
    tok_cp.start()
    loads = [
        pltpu.make_async_copy(src, dst, loc_s.at[1 + n])
        for n, (src, dst) in enumerate(
            ((wk_hbm, wk), (wv_hbm, wv), (wq_hbm, wq), (wg_hbm, wg), (wo_hbm, wo))
        )
    ]
    for cp in loads:
        cp.start()

    barrier = pltpu.get_barrier_semaphore()

    def greet_plane(n, carry):
        for core in range(2):
            who = y * 2 + core

            @pl.when(jnp.logical_or(n != sp, core != c))
            def _():
                pl.semaphore_signal(barrier, inc=1, device_id=(n, who), device_id_type=MESH)

        return carry

    lax.fori_loop(0, NZ * NX, greet_plane, 0)
    for dy in range(1, NY):
        yy = (y + dy) % NY
        for xx in range(NX):
            pl.semaphore_signal(
                barrier, inc=1, device_id=(z * NX + xx, yy * 2 + c), device_id_type=MESH
            )
        pl.semaphore_signal(
            barrier, inc=1, device_id=(sp, yy * 2 + (1 - c)), device_id_type=MESH
        )
    tok_cp.wait()
    pl.semaphore_wait(barrier, 2 * NZ * NX - 1 + (NY - 1) * (NX + 1))

    def half(h):
        return pl.ds(pl.multiple_of(c * ROW + h * (ROW // 2), ROW // 2), ROW // 2)

    def tok_up(h):
        return rcopy(tok.at[0, half(h)], tok.at[2, half(h)], ty_s.at[0, h], ty_r.at[0, h], sp, ynext)

    def tok_down(h):
        return rcopy(tok.at[0, half(h)], tok.at[1, half(h)], ty_s.at[1, h], ty_r.at[1, h], sp, yprev)

    def relay_up():
        return rcopy(tok.at[2, half(0)], tok.at[3, half(0)], tr_s.at[0], tr_r.at[0], sp, ynext)

    def relay_down():
        return rcopy(tok.at[1, half(1)], tok.at[3, half(1)], tr_s.at[1], tr_r.at[1], sp, yprev)

    def tok_pair(i):
        return rcopy(tok.at[i, mine], tok.at[i, mine], tp_s.at[i], tp_r.at[i], sp, other)

    def wait_pair(i):
        theirs = pl.ds(pl.multiple_of((1 - c) * ROW, ROW), ROW)
        rcopy(tok.at[i, theirs], tok.at[i, theirs], tp_s.at[i], tp_r.at[i], sp, other).wait_recv()

    tok_up(0).start()
    tok_down(1).start()
    tok_pair(0).start()
    tok_up(1).start()
    tok_down(0).start()

    mx[...] = jnp.full_like(mx, -1e30)
    ln[...] = jnp.zeros_like(ln)
    acc[...] = jnp.zeros_like(acc)

    own_head = x // 2 == c
    own_j = x - 2 * c

    def x_kv(i, j, r):
        rows = pl.ds(r * ROW, ROW)
        return rcopy(
            kvs.at[i, j, :, rows], kv.at[z, i, :, x, rows], xk_s.at[i, j, r], xk_r.at[i, x],
            z * NX + 2 * c + j, y * 2 + r,
        )

    def x_q(i, j, r):
        rows = pl.ds(r * ROW, ROW)
        return rcopy(
            qs.at[i, j, rows], q.at[x, i], xq_s.at[i, j, r], xq_r.at[i, x],
            z * NX + 2 * c + j, y * 2 + r,
        )

    def gate_copy(i, cc):
        yy = (y + DELTA[i]) % NY
        return rcopy(
            gbuf.at[i, pl.ds(cc * ROW, ROW)], ggot.at[tp], g_s.at[i, cc], g_r.at[tp], sp, yy * 2 + cc
        )

    def away(j, r):
        return jnp.logical_or(x != 2 * c + j, c != r)

    def project(i):
        part = tok[i]
        k = jnp.dot(part, wk[...], preferred_element_type=F32).astype(BF16)
        v = jnp.dot(part, wv[...], preferred_element_type=F32).astype(BF16)
        for j in range(2):
            kvs[i, j, 0] = k[:, j * HD : (j + 1) * HD]
            kvs[i, j, 1] = v[:, j * HD : (j + 1) * HD]
        for j in range(2):
            for r in range(2):

                @pl.when(away(j, r))
                def _():
                    x_kv(i, j, r).start()

        qq = (jnp.dot(part, wq[...], preferred_element_type=F32) * HD ** (-0.5)).astype(BF16)
        for j in range(2):
            qs[i, j] = qq[:, j * HD : (j + 1) * HD]
        for j in range(2):
            for r in range(2):

                @pl.when(away(j, r))
                def _():
                    x_q(i, j, r).start()

        for j in range(2):

            @pl.when(x == 2 * c + j)
            def _():
                kv[z, i, :, x, mine] = kvs[i, j, :, mine]
                q[x, i] = qs[i, j, mine]

        gate = jax.nn.sigmoid(jnp.dot(part, wg[...], preferred_element_type=F32))
        gbuf[i] = gate
        for cc in range(2):
            if i == 0:

                @pl.when(c != cc)
                def _():
                    gate_copy(i, cc).start()

                @pl.when(c == cc)
                def _():
                    ggot[tp] = gbuf[i, cc * ROW : (cc + 1) * ROW]
            else:
                gate_copy(i, cc).start()
        logits = jnp.dot(part, fw_ref[...], preferred_element_type=F32) + fb_ref[...]
        small = jnp.exp(-jnp.abs(logits))
        grown = 1.0 + small
        tail = jnp.where(grown == 1.0, small, jnp.log(grown) * (small / jnp.where(grown == 1.0, 1.0, grown - 1.0)))
        logs = jnp.minimum(logits, 0.0) - tail
        pick = (
            lax.broadcasted_iota(jnp.int32, (8, 16), 1)
            == lax.broadcasted_iota(jnp.int32, (8, 16), 0) + 2 * tp
        ).astype(F32)
        turned = lax.dot_general(pick, logs, NT, precision=lax.Precision.HIGHEST, preferred_element_type=F32)
        tri = (
            lax.broadcasted_iota(jnp.int32, (SUB, SUB), 0) <= lax.broadcasted_iota(jnp.int32, (SUB, SUB), 1)
        ).astype(F32)
        summed = jnp.dot(turned, tri, precision=lax.Precision.HIGHEST, preferred_element_type=F32)
        yy = (y + DELTA[i]) % NY
        lg[:, pl.ds(pl.multiple_of(yy * SUB, SUB), SUB)] = summed

    def z_up(o, p, t):
        ref = kv.at[o, p, :, :, mine]
        return rcopy(ref, ref, zs.at[0, t], zr.at[0, t], up, tp)

    def z_down(o, p, t):
        ref = kv.at[o, p, :, :, mine]
        return rcopy(ref, ref, zs.at[1, t], zr.at[1, t], down, tp)

    def z_pair(o, p, way, t):
        ref = kv.at[o, p, :, :, mine]
        return rcopy(ref, ref, ps.at[way, t], pr.at[way, t], sp, other)

    def own_pair(p):
        ref = kv.at[z, p, :, :, mine]
        return rcopy(ref, ref, po_s.at[p], po_r.at[p], sp, other)

    def reach(way, p):
        return 3 + (p < 2).astype(jnp.int32) if way == 0 else 3 + (p >= 2).astype(jnp.int32)

    def goes(way, o, p, d):
        far = reach(way, p)
        if way == 0:
            return jnp.logical_and(d <= far, o + d < NZ)
        return jnp.logical_and(d <= far, o + 1 <= far)

    def first_sends(p):
        for xs in range(NX):

            @pl.when(jnp.logical_not(jnp.logical_and(own_head, x == xs)))
            def _():
                ref = kv.at[z, p, :, xs, mine]
                rcopy(ref, ref, xk_s.at[p, 0, 0], xk_r.at[p, xs], sp, other).wait_recv()

        pv = jnp.int32(p)

        @pl.when(goes(0, z, pv, 1))
        def _():
            z_up(z, p, p).start()

        @pl.when(goes(1, z, pv, 1))
        def _():
            z_down(z, p, p).start()

        own_pair(p).start()

    for cp in loads[:4]:
        cp.wait()
    wait_pair(0)
    project(0)
    tok_up(0).wait_recv()
    relay_up().start()
    tok_down(1).wait_recv()
    relay_down().start()
    first_sends(0)
    tok_up(1).wait_recv()
    tok_pair(2).start()
    tok_down(0).wait_recv()
    tok_pair(1).start()
    wait_pair(2)
    project(2)
    wait_pair(1)
    project(1)
    relay_up().wait_recv()
    relay_down().wait_recv()
    tok_pair(3).start()
    first_sends(2)
    first_sends(1)
    wait_pair(3)
    project(3)

    past = jnp.zeros((8, 1), F32)
    for yy in range(NY):
        piece = lg[:, yy * SUB : (yy + 1) * SUB] + past
        past = piece[:, SUB - 1 : SUB]
        for j in range(2):
            lcs[j, :, yy * SUB : (yy + 1) * SUB] = piece[j : j + 1]

    def log_copy(zz, j, r):
        return rcopy(lcs.at[j], lcbuf.at[sp], l_s.at[zz, j, r], l_r.at[sp], zz * NX + 2 * c + j, y * 2 + r)

    def log_away(zz, j, r):
        return jnp.logical_or(z != zz, away(j, r))

    def send_logs(zz, carry):
        for j in range(2):
            for r in range(2):

                @pl.when(log_away(zz, j, r))
                def _():
                    log_copy(zz, j, r).start()

        return carry

    lax.fori_loop(0, NZ, send_logs, 0)
    for j in range(2):

        @pl.when(x == 2 * c + j)
        def _():
            lcbuf[sp] = lcs[j]

    first_sends(3)

    def origin(way, d):
        return z - d if way == 0 else (z + d) % NZ

    def arrives(way, t):
        d, p = t // 4 + 1, t % 4
        o = origin(way, d)
        return jnp.logical_and(o >= 0, goes(way, o, p, d))

    def relay(t):
        d, p = t // 4 + 1, t % 4
        for way, hop in ((0, z_up), (1, z_down)):
            o = origin(way, d)

            @pl.when(arrives(way, t))
            def _():
                hop(o, p, t).wait_recv()

                @pl.when(goes(way, o, p, d + 1))
                def _():
                    hop(o, p, t + 4).start()

                @pl.when(o < z)
                def _():
                    z_pair(o, p, way, t).start()

    def attend(o, p, diagonal):
        keys = kv[o, p, 0].reshape(NX * SUB, HD)
        values = kv[o, p, 1].reshape(NX * SUB, HD)
        g = p % 4
        yy = (y + g + (g == 2).astype(jnp.int32) - (g == 3).astype(jnp.int32)) % NY
        bias = cu[o, yy]

        def block(b, carry):
            s = lax.dot_general(q[b].reshape(256, HD), keys, NT, preferred_element_type=F32) - bias
            if diagonal:
                row = lax.broadcasted_iota(jnp.int32, (256, 1), 0)
                turn = row >> 6
                turn = turn ^ (turn >> 1)
                at_q = b * 512 + ((turn + y) & 3) * SUB + c * ROW + (row & 63)
                lane = lax.broadcasted_iota(jnp.int32, (1, NX * SUB), 1)
                at_k = (lane >> 7) * 512 + yy * SUB + (lane & 127)
                s = jnp.where(at_k <= at_q, s, -jnp.inf)
            old = mx[b]
            new = jnp.maximum(old, jnp.max(s, axis=1, keepdims=True))
            factor = jnp.exp(old - new)
            weights = [jnp.exp(s[:, n * 128 : (n + 1) * 128] - new) for n in range(NX)]
            ln[b] = ln[b] * factor + ((weights[0] + weights[1]) + (weights[2] + weights[3]))
            rounded = jnp.concatenate([w.astype(BF16) for w in weights], axis=1)
            acc[b] = acc[b] * factor + jnp.dot(rounded, values, preferred_element_type=F32)
            mx[b] = new
            return carry

        lax.fori_loop(0, NX, block, 0)

    relay(jnp.int32(0))

    for n in range(NZ * NX):

        @pl.when(jnp.logical_not(jnp.logical_and(own_head, sp == n)))
        def _():
            ref = lcbuf.at[n]
            rcopy(ref, ref, l_s.at[0, 0, 0], l_r.at[n], sp, other).wait_recv()

    base = jnp.zeros((1, 1), F32)
    for n in range(NZ * NX):
        base = base + jnp.where(n < NX * z, lcbuf[n, :, 511:512], 0.0)
    offset = -base
    for n in range(NZ * NX):
        line = lcbuf[n] + offset
        for yy in range(NY):
            cu[n // NX, yy, :, (n % NX) * SUB : (n % NX + 1) * SUB] = line[:, yy * SUB : (yy + 1) * SUB]
        offset = offset + lcbuf[n, :, 511:512]

    for i in range(NY):
        for xs in range(NX):

            @pl.when(jnp.logical_not(jnp.logical_and(own_head, x == xs)))
            def _():
                ref = q.at[xs, i]
                rcopy(ref, ref, xq_s.at[i, 0, 0], xq_r.at[i, xs], sp, other).wait_recv()

    theirs = pl.ds(pl.multiple_of((1 - c) * ROW, ROW), ROW)

    def pair_wait(o, p, sem):
        ref = kv.at[o, p, :, :, theirs]
        rcopy(ref, ref, po_s.at[0], sem, sp, other).wait_recv()

    def consume(t):
        d, p = t // 4 + 1, t % 4
        for way in range(2):
            o = origin(way, d)

            @pl.when(jnp.logical_and(arrives(way, t), o < z))
            def _():
                pair_wait(o, p, pr.at[way, t])
                attend(o, p, False)

    def step(t, carry):
        @pl.when(t < 15)
        def _():
            relay(t + 1)

        @pl.when(t < 4)
        def _():
            pair_wait(z, t, po_r.at[t])
            attend(z, t, True)

        consume(t)
        return carry

    lax.fori_loop(0, 16, step, 0)

    head = y * NX + x

    def out_copy(b, i):
        yy = (y + DELTA[i]) % NY
        return rcopy(ob.at[b, i], obuf.at[head], o_s.at[b, i], o_r.at[head], z * NX + b, yy * 2 + c)

    for b in range(NX):
        done = acc[b] / jnp.sum(ln[b], axis=1, keepdims=True)
        ob[b] = done.astype(BF16).reshape(NY, ROW, HD)
        for i in range(NY):
            if i == 0:

                @pl.when(x != b)
                def _():
                    out_copy(b, i).start()

                @pl.when(x == b)
                def _():
                    obuf[head] = ob[b, i]
            else:
                out_copy(b, i).start()

    loads[4].wait()
    for n in range(8):

        @pl.when(tp != n)
        def _():
            ref = ggot.at[n]
            rcopy(ref, ref, g_s.at[0, 0], g_r.at[n], sp, other).wait_recv()

    for h in range(NX * NY):

        @pl.when(head != h)
        def _():
            ref = obuf.at[h]
            rcopy(ref, ref, o_s.at[0, 0], o_r.at[h], sp, other).wait_recv()

        cols = slice((h % 2) * HD, (h % 2 + 1) * HD)
        att[:, h * HD : (h + 1) * HD] = (obuf[h].astype(F32) * ggot[h // 2][:, cols]).astype(BF16)

    for n in range(4):
        cols = slice(n * 512, (n + 1) * 512)
        out_ref[:, cols] = jnp.dot(att[...], wo[:, cols], preferred_element_type=F32).astype(BF16)

    for h in range(2):
        tok_up(h).wait_send()
        tok_down(h).wait_send()
    relay_up().wait_send()
    relay_down().wait_send()
    for i in range(NY):
        tok_pair(i).wait_send()
        own_pair(i).wait_send()
        for j in range(2):
            for r in range(2):

                @pl.when(away(j, r))
                def _():
                    x_kv(i, j, r).wait_send()
                    x_q(i, j, r).wait_send()

        for cc in range(2):

            @pl.when(jnp.logical_or(i != 0, c != cc))
            def _():
                gate_copy(i, cc).wait_send()

        for b in range(NX):

            @pl.when(jnp.logical_or(i != 0, x != b))
            def _():
                out_copy(b, i).wait_send()

    def drain_logs(zz, carry):
        for j in range(2):
            for r in range(2):

                @pl.when(log_away(zz, j, r))
                def _():
                    log_copy(zz, j, r).wait_send()

        return carry

    lax.fori_loop(0, NZ, drain_logs, 0)

    def drain(t, carry):
        d, p = t // 4 + 1, t % 4
        for way, hop in ((0, z_up), (1, z_down)):
            src = origin(way, d - 1)

            @pl.when(jnp.logical_and(src >= 0, goes(way, src, p, d)))
            def _():
                hop(src, p, t).wait_send()

            o = origin(way, d)

            @pl.when(jnp.logical_and(arrives(way, t), o < z))
            def _():
                z_pair(o, p, way, t).wait_send()

        return carry

    lax.fori_loop(0, 16, drain, 0)


def body(tokens, query_weight, key_weight, value_weight, gate_weight, forget_weight, forget_bias, out_weight):
    dma = pltpu.SemaphoreType.DMA
    vmem = pltpu.VMEM
    anywhere = pl.BlockSpec(memory_space=pl.ANY)
    local = pl.BlockSpec(memory_space=pltpu.VMEM)
    return pl.pallas_call(
        kernel,
        out_shape=jax.ShapeDtypeStruct((ROW, D), BF16),
        in_specs=[anywhere] * 5 + [local, local, anywhere],
        out_specs=local,
        scratch_shapes=[
            vmem((NY, SUB, D), BF16),
            vmem((D, WIDTH), BF16),
            vmem((D, WIDTH), BF16),
            vmem((D, WIDTH), BF16),
            vmem((D, WIDTH), BF16),
            vmem((D, D), BF16),
            vmem((NY, 2, 2, SUB, HD), BF16),
            vmem((NY, 2, SUB, HD), BF16),
            vmem((NY, SUB, WIDTH), F32),
            vmem((8, ROW, WIDTH), F32),
            vmem((8, 512), F32),
            vmem((2, 1, 512), F32),
            vmem((NZ * NX, 1, 512), F32),
            vmem((NZ, NY, 1, 512), F32),
            vmem((NZ, NY, 2, NX, SUB, HD), BF16),
            vmem((NX, NY, ROW, HD), BF16),
            vmem((NX, 256, HD), F32),
            vmem((NX, 256, HD), F32),
            vmem((NX, 256, HD), F32),
            vmem((NX, NY, ROW, HD), BF16),
            vmem((16, ROW, HD), BF16),
            vmem((ROW, D), BF16),
            dma((6,)),
            dma((2, 2)), dma((2, 2)), dma((2,)), dma((2,)), dma((4,)), dma((4,)),
            dma((4, 2, 2)), dma((4, 4)), dma((4, 2, 2)), dma((4, 4)),
            dma((4, 2)), dma((8,)),
            dma((8, 2, 2)), dma((32,)),
            dma((4, 4)), dma((16,)),
            dma((2, 16)), dma((2, 16)), dma((2, 16)), dma((2, 16)), dma((4,)), dma((4,)),
        ],
        compiler_params=pltpu.CompilerParams(
            collective_id=0, has_side_effects=True, vmem_limit_bytes=60 * 1024 * 1024
        ),
    )(
        tokens, query_weight, key_weight, value_weight, gate_weight,
        forget_weight, forget_bias.reshape(1, 16), out_weight,
    )


def solution(mesh):
    placed = (
        P(("sp", "tp"), None), P(None, "tp"), P(None, "tp"), P(None, "tp"), P(None, "tp"), P(), P(), P(),
    )
    return jax.shard_map(
        body, mesh=mesh, in_specs=placed, out_specs=P(("sp", "tp"), None), check_vma=False
    )
```

```python
import jax
import jax.numpy as jnp
from jax import lax
from jax.experimental import pallas as pl
from jax.experimental.pallas import tpu as pltpu
from jax.sharding import PartitionSpec as P

NZ, NX, NY = 8, 4, 4
HD = 128
WIDTH = 256
D = 2048
SUB = 128
ROW = 64
DELTA = (0, 1, 3, 2)
MESH = pl.DeviceIdType.MESH
NT = (((1,), (1,)), ((), ()))
F32, BF16 = jnp.float32, jnp.bfloat16
LOG2E = 1.4426950408889634


def rcopy(src, dst, send, recv, sp, tp):
    return pltpu.make_async_remote_copy(
        src_ref=src,
        dst_ref=dst,
        send_sem=send,
        recv_sem=recv,
        device_id=(sp, tp),
        device_id_type=MESH,
    )


def kernel(
    tok_hbm, wq_hbm, wk_hbm, wv_hbm, wg_hbm, fw_ref, fb_ref, wo_hbm, out_ref,
    tok, wq, wk, wv, wg, wo, kvs, qs, gbuf, ggot, lg, lcs, lcbuf, cu, kv, q, acc, mx, ln, ob, obuf, att,
    loc_s, ty_s, ty_r, tr_s, tr_r, tp_s, tp_r,
    xk_s, xk_r, xq_s, xq_r, g_s, g_r, l_s, l_r, lz_s, lz_r, o_s, o_r,
    zs, zr, ps, pr, po_s, po_r,
):
    sp = lax.axis_index("sp")
    tp = lax.axis_index("tp")
    z, x = sp // NX, sp % NX
    y, c = tp // 2, tp % 2
    other = y * 2 + (1 - c)
    up = ((z + 1) % NZ) * NX + x
    down = ((z + NZ - 1) % NZ) * NX + x
    ynext = ((y + 1) % NY) * 2 + c
    yprev = ((y + NY - 1) % NY) * 2 + c
    mine = pl.ds(pl.multiple_of(c * ROW, ROW), ROW)

    tok_cp = pltpu.make_async_copy(tok_hbm, tok.at[0, mine], loc_s.at[0])
    tok_cp.start()
    loads = [
        pltpu.make_async_copy(src, dst, loc_s.at[1 + n])
        for n, (src, dst) in enumerate(
            ((wk_hbm, wk), (wv_hbm, wv), (wq_hbm, wq), (wg_hbm, wg), (wo_hbm, wo))
        )
    ]
    for cp in loads[:4]:
        cp.start()

    barrier = pltpu.get_barrier_semaphore()

    def greet(who_sp, who_tp):
        pl.semaphore_signal(barrier, inc=1, device_id=(who_sp, who_tp), device_id_type=MESH)

    greet(sp, other)
    for dy in range(1, NY):
        for core in range(2):
            greet(sp, ((y + dy) % NY) * 2 + core)
    for dz in range(1, NZ):
        greet(((z + dz) % NZ) * NX + x, tp)
    for dx in range(1, NX):
        xx = z * NX + (x + dx) % NX
        for core in range(2):
            greet(xx, y * 2 + core)
        for dy in range(1, NY):
            greet(xx, ((y + dy) % NY) * 2 + c)
    tok_cp.wait()
    pl.semaphore_wait(barrier, 2 * NY - 1 + NZ - 1 + (NX - 1) * (NY + 1))

    def half(h):
        return pl.ds(pl.multiple_of(c * ROW + h * (ROW // 2), ROW // 2), ROW // 2)

    def tok_up(h):
        return rcopy(tok.at[0, half(h)], tok.at[2, half(h)], ty_s.at[0, h], ty_r.at[0, h], sp, ynext)

    def tok_down(h):
        return rcopy(tok.at[0, half(h)], tok.at[1, half(h)], ty_s.at[1, h], ty_r.at[1, h], sp, yprev)

    def relay_up():
        return rcopy(tok.at[2, half(0)], tok.at[3, half(0)], tr_s.at[0], tr_r.at[0], sp, ynext)

    def relay_down():
        return rcopy(tok.at[1, half(1)], tok.at[3, half(1)], tr_s.at[1], tr_r.at[1], sp, yprev)

    def tok_pair(i):
        return rcopy(tok.at[i, mine], tok.at[i, mine], tp_s.at[i], tp_r.at[i], sp, other)

    def wait_pair(i):
        theirs = pl.ds(pl.multiple_of((1 - c) * ROW, ROW), ROW)
        rcopy(tok.at[i, theirs], tok.at[i, theirs], tp_s.at[i], tp_r.at[i], sp, other).wait_recv()

    tok_up(0).start()
    tok_down(1).start()
    tok_pair(0).start()
    tok_up(1).start()
    tok_down(0).start()

    mx[...] = jnp.full_like(mx, -1e30)
    ln[...] = jnp.zeros_like(ln)
    acc[...] = jnp.zeros_like(acc)

    own_head = x // 2 == c
    own_j = x - 2 * c

    def x_kv(i, j, r):
        rows = pl.ds(r * ROW, ROW)
        return rcopy(
            kvs.at[i, j, :, rows], kv.at[z, i, :, x, rows], xk_s.at[i, j, r], xk_r.at[i, x],
            z * NX + 2 * c + j, y * 2 + r,
        )

    def x_q(i, j, r):
        rows = pl.ds(r * ROW, ROW)
        return rcopy(
            qs.at[i, j, rows], q.at[x, i], xq_s.at[i, j, r], xq_r.at[i, x],
            z * NX + 2 * c + j, y * 2 + r,
        )

    def gate_copy(i, cc):
        yy = (y + DELTA[i]) % NY
        return rcopy(
            gbuf.at[i, pl.ds(cc * ROW, ROW)], ggot.at[tp], g_s.at[i, cc], g_r.at[tp], sp, yy * 2 + cc
        )

    def away(j, r):
        return jnp.logical_or(x != 2 * c + j, c != r)

    def project(i):
        part = tok[i]
        k = jnp.dot(part, wk[...], preferred_element_type=F32).astype(BF16)
        v = jnp.dot(part, wv[...], preferred_element_type=F32).astype(BF16)
        for j in range(2):
            kvs[i, j, 0] = k[:, j * HD : (j + 1) * HD]
            kvs[i, j, 1] = v[:, j * HD : (j + 1) * HD]
        for j in range(2):
            for r in range(2):

                @pl.when(away(j, r))
                def _():
                    x_kv(i, j, r).start()

        qq = (jnp.dot(part, wq[...], preferred_element_type=F32) * HD ** (-0.5)).astype(BF16)
        for j in range(2):
            qs[i, j] = qq[:, j * HD : (j + 1) * HD]
        for j in range(2):
            for r in range(2):

                @pl.when(away(j, r))
                def _():
                    x_q(i, j, r).start()

        for j in range(2):

            @pl.when(x == 2 * c + j)
            def _():
                kv[z, i, :, x, mine] = kvs[i, j, :, mine]
                q[x, i] = qs[i, j, mine]

        gate = jax.nn.sigmoid(jnp.dot(part, wg[...], preferred_element_type=F32))
        gbuf[i] = gate
        for cc in range(2):
            if i == 0:

                @pl.when(c != cc)
                def _():
                    gate_copy(i, cc).start()

                @pl.when(c == cc)
                def _():
                    ggot[tp] = gbuf[i, cc * ROW : (cc + 1) * ROW]
            else:
                gate_copy(i, cc).start()
        diag = lax.broadcasted_iota(jnp.int32, (16, 16), 0) == lax.broadcasted_iota(jnp.int32, (16, 16), 1)
        bias = jnp.sum(jnp.where(diag, fb_ref[...], 0.0), axis=1, keepdims=True)
        logits = lax.dot_general(fw_ref[...], part, NT, preferred_element_type=F32) + bias
        small = jnp.exp(-jnp.abs(logits))
        grown = 1.0 + small
        tail = jnp.where(grown == 1.0, small, jnp.log(grown) * (small / jnp.where(grown == 1.0, 1.0, grown - 1.0)))
        logs = jnp.minimum(logits, 0.0) - tail
        pick = (
            lax.broadcasted_iota(jnp.int32, (8, 16), 1)
            == lax.broadcasted_iota(jnp.int32, (8, 16), 0) + 2 * tp
        ).astype(F32)
        turned = jnp.dot(pick, logs, precision=lax.Precision.HIGHEST, preferred_element_type=F32)
        tri = (
            lax.broadcasted_iota(jnp.int32, (SUB, SUB), 0) <= lax.broadcasted_iota(jnp.int32, (SUB, SUB), 1)
        ).astype(F32)
        summed = jnp.dot(turned, tri, precision=lax.Precision.HIGHEST, preferred_element_type=F32)
        yy = (y + DELTA[i]) % NY
        lg[:, pl.ds(pl.multiple_of(yy * SUB, SUB), SUB)] = summed

    def z_up(o, p, t):
        ref = kv.at[o, p, :, :, mine]
        return rcopy(ref, ref, zs.at[0, t], zr.at[0, t], up, tp)

    def z_down(o, p, t):
        ref = kv.at[o, p, :, :, mine]
        return rcopy(ref, ref, zs.at[1, t], zr.at[1, t], down, tp)

    def z_pair(o, p, way, t):
        ref = kv.at[o, p, :, :, mine]
        return rcopy(ref, ref, ps.at[way, t], pr.at[way, t], sp, other)

    def own_pair(p):
        ref = kv.at[z, p, :, :, mine]
        return rcopy(ref, ref, po_s.at[p], po_r.at[p], sp, other)

    def reach(way, p):
        return 3 + (p < 2).astype(jnp.int32) if way == 0 else 3 + (p >= 2).astype(jnp.int32)

    def goes(way, o, p, d):
        far = reach(way, p)
        if way == 0:
            return jnp.logical_and(d <= far, o + d < NZ)
        return jnp.logical_and(d <= far, o + 1 <= far)

    def first_sends(p):
        for xs in range(NX):

            @pl.when(jnp.logical_not(jnp.logical_and(own_head, x == xs)))
            def _():
                ref = kv.at[z, p, :, xs, mine]
                rcopy(ref, ref, xk_s.at[p, 0, 0], xk_r.at[p, xs], sp, other).wait_recv()

        pv = jnp.int32(p)

        @pl.when(goes(0, z, pv, 1))
        def _():
            z_up(z, p, p).start()

        @pl.when(goes(1, z, pv, 1))
        def _():
            z_down(z, p, p).start()

        own_pair(p).start()

    for cp in loads[:4]:
        cp.wait()
    wait_pair(0)
    project(0)
    loads[4].start()
    tok_up(0).wait_recv()
    relay_up().start()
    tok_down(1).wait_recv()
    relay_down().start()
    first_sends(0)
    tok_up(1).wait_recv()
    tok_pair(2).start()
    tok_down(0).wait_recv()
    tok_pair(1).start()
    wait_pair(2)
    project(2)
    wait_pair(1)
    project(1)
    first_sends(2)
    relay_up().wait_recv()
    relay_down().wait_recv()
    tok_pair(3).start()
    first_sends(1)
    wait_pair(3)
    project(3)

    past = jnp.zeros((8, 1), F32)
    for yy in range(NY):
        piece = lg[:, yy * SUB : (yy + 1) * SUB] + past
        past = piece[:, SUB - 1 : SUB]
        for j in range(2):
            lcs[j, :, yy * SUB : (yy + 1) * SUB] = piece[j : j + 1]

    def log_copy(j, r):
        return rcopy(lcs.at[j], lcbuf.at[sp], l_s.at[j, r], l_r.at[x], z * NX + 2 * c + j, y * 2 + r)

    for j in range(2):
        for r in range(2):

            @pl.when(away(j, r))
            def _():
                log_copy(j, r).start()

        @pl.when(x == 2 * c + j)
        def _():
            lcbuf[sp] = lcs[j]

    first_sends(3)

    def origin(way, d):
        return z - d if way == 0 else (z + d) % NZ

    def arrives(way, t):
        d, p = t // 4 + 1, t % 4
        o = origin(way, d)
        return jnp.logical_and(o >= 0, goes(way, o, p, d))

    def relay(t):
        d, p = t // 4 + 1, t % 4
        for way, hop in ((0, z_up), (1, z_down)):
            o = origin(way, d)

            @pl.when(arrives(way, t))
            def _():
                hop(o, p, t).wait_recv()

                @pl.when(goes(way, o, p, d + 1))
                def _():
                    hop(o, p, t + 4).start()

                @pl.when(o < z)
                def _():
                    z_pair(o, p, way, t).start()

    def slot(p):
        g = p % 4
        return (y + g + (g == 2).astype(jnp.int32) - (g == 3).astype(jnp.int32)) % NY

    def attend(origins, p, diagonal):
        yy = slot(p)
        rows = q[...].reshape(NX * 256, HD)
        scores = [
            lax.dot_general(rows, kv[o, p, 0].reshape(NX * SUB, HD), NT, preferred_element_type=F32)
            for o in origins
        ]
        biases = [cu[o, yy] for o in origins]
        rounded, factors = [], []
        for b in range(NX):
            parts = []
            for score, bias in zip(scores, biases):
                s = score[b * 256 : (b + 1) * 256] * LOG2E - bias
                if diagonal:
                    row = lax.broadcasted_iota(jnp.int32, (256, 1), 0)
                    turn = row >> 6
                    turn = turn ^ (turn >> 1)
                    at_q = b * 512 + ((turn + y) & 3) * SUB + c * ROW + (row & 63)
                    lane = lax.broadcasted_iota(jnp.int32, (1, NX * SUB), 1)
                    at_k = (lane >> 7) * 512 + yy * SUB + (lane & 127)
                    s = jnp.where(at_k <= at_q, s, -jnp.inf)
                parts.append(s)
            old = mx[b]
            new = old
            for s in parts:
                new = jnp.maximum(new, jnp.max(s, axis=1, keepdims=True))
            factor = jnp.exp2(old - new)
            weights = [jnp.exp2(s[:, n * 128 : (n + 1) * 128] - new) for s in parts for n in range(NX)]
            sums = weights
            while len(sums) > 1:
                sums = [sums[n] + sums[n + 1] for n in range(0, len(sums), 2)]
            ln[b] = ln[b] * factor + sums[0]
            rounded.append(jnp.concatenate([w.astype(BF16) for w in weights], axis=1))
            factors.append(factor)
            mx[b] = new
        values = [kv[o, p, 1].reshape(NX * SUB, HD) for o in origins]
        values = values[0] if len(values) == 1 else jnp.concatenate(values, axis=0)
        more = jnp.dot(jnp.concatenate(rounded, axis=0), values, preferred_element_type=F32)
        for b in range(NX):
            acc[b] = acc[b] * factors[b] + more[b * 256 : (b + 1) * 256]

    for xs in range(NX):

        @pl.when(jnp.logical_not(jnp.logical_and(own_head, x == xs)))
        def _():
            ref = lcbuf.at[z * NX + xs]
            rcopy(ref, ref, l_s.at[0, 0], l_r.at[xs], sp, other).wait_recv()

    def z_logs(dz):
        ref = lcbuf.at[pl.ds(z * NX, NX)]
        return rcopy(ref, ref, lz_s.at[dz], lz_r.at[z], ((z + dz) % NZ) * NX + x, tp)

    for dz in range(1, NZ):
        z_logs(dz).start()

    offset = jnp.zeros((1, 1), F32)
    for n in range(NX):
        line = lcbuf[z * NX + n]
        scaled = (line + offset) * LOG2E
        for yy in range(NY):
            cu[z, yy, :, n * SUB : (n + 1) * SUB] = scaled[:, yy * SUB : (yy + 1) * SUB]
        offset = offset + line[:, 511:512]

    relay(jnp.int32(0))

    for i in range(NY):
        for xs in range(NX):

            @pl.when(jnp.logical_not(jnp.logical_and(own_head, x == xs)))
            def _():
                ref = q.at[xs, i]
                rcopy(ref, ref, xq_s.at[i, 0, 0], xq_r.at[i, xs], sp, other).wait_recv()

    theirs = pl.ds(pl.multiple_of((1 - c) * ROW, ROW), ROW)

    def pair_wait(o, p, sem):
        ref = kv.at[o, p, :, :, theirs]
        rcopy(ref, ref, po_s.at[0], sem, sp, other).wait_recv()

    def consume(t):
        d, p = t // 4 + 1, t % 4
        ups = arrives(0, t)
        o_up, o_down = origin(0, d), origin(1, d)
        downs = jnp.logical_and(arrives(1, t), o_down < z)

        @pl.when(ups)
        def _():
            pair_wait(o_up, p, pr.at[0, t])

        @pl.when(downs)
        def _():
            pair_wait(o_down, p, pr.at[1, t])

        @pl.when(jnp.logical_and(ups, downs))
        def _():
            attend([o_up, o_down], p, False)

        @pl.when(jnp.logical_xor(ups, downs))
        def _():
            attend([jnp.where(ups, o_up, o_down)], p, False)

    relay(jnp.int32(1))

    def own_piece(t, carry):
        @pl.when(t >= 2)
        def _():
            relay(t)

        pair_wait(z, t, po_r.at[t])
        attend([z], t, True)
        return carry

    lax.fori_loop(0, 4, own_piece, 0)

    for n in range(NZ):

        @pl.when(z != n)
        def _():
            ref = lcbuf.at[pl.ds(n * NX, NX)]
            rcopy(ref, ref, lz_s.at[1], lz_r.at[n], sp, other).wait_recv()

    base = jnp.zeros((1, 1), F32)
    for n in range(NZ * NX):
        base = base + jnp.where(n < NX * z, lcbuf[n, :, 511:512], 0.0)
    offset = -base
    for n in range(NZ * NX):
        line = lcbuf[n]
        scaled = (line + offset) * LOG2E
        for yy in range(NY):
            cu[n // NX, yy, :, (n % NX) * SUB : (n % NX + 1) * SUB] = scaled[:, yy * SUB : (yy + 1) * SUB]
        offset = offset + line[:, 511:512]

    def step(t, carry):
        @pl.when(jnp.logical_and(t >= 3, t < 15))
        def _():
            relay(t + 1)

        consume(t)
        return carry

    lax.fori_loop(0, 16, step, 0)

    head = y * NX + x

    def out_copy(b, i):
        yy = (y + DELTA[i]) % NY
        return rcopy(ob.at[b, i], obuf.at[head], o_s.at[b, i], o_r.at[head], z * NX + b, yy * 2 + c)

    for b in range(NX):
        done = acc[b] / jnp.sum(ln[b], axis=1, keepdims=True)
        ob[b] = done.astype(BF16).reshape(NY, ROW, HD)
        for i in range(NY):
            if i == 0:

                @pl.when(x != b)
                def _():
                    out_copy(b, i).start()

                @pl.when(x == b)
                def _():
                    obuf[head] = ob[b, i]
            else:
                out_copy(b, i).start()

    loads[4].wait()
    for n in range(8):

        @pl.when(tp != n)
        def _():
            ref = ggot.at[n]
            rcopy(ref, ref, g_s.at[0, 0], g_r.at[n], sp, other).wait_recv()

    for h in range(NX * NY):

        @pl.when(head != h)
        def _():
            ref = obuf.at[h]
            rcopy(ref, ref, o_s.at[0, 0], o_r.at[h], sp, other).wait_recv()

        cols = slice((h % 2) * HD, (h % 2 + 1) * HD)
        att[:, h * HD : (h + 1) * HD] = (obuf[h].astype(F32) * ggot[h // 2][:, cols]).astype(BF16)

    for n in range(4):
        cols = slice(n * 512, (n + 1) * 512)
        out_ref[:, cols] = jnp.dot(att[...], wo[:, cols], preferred_element_type=F32).astype(BF16)

    for h in range(2):
        tok_up(h).wait_send()
        tok_down(h).wait_send()
    relay_up().wait_send()
    relay_down().wait_send()
    for i in range(NY):
        tok_pair(i).wait_send()
        own_pair(i).wait_send()
        for j in range(2):
            for r in range(2):

                @pl.when(away(j, r))
                def _():
                    x_kv(i, j, r).wait_send()
                    x_q(i, j, r).wait_send()

        for cc in range(2):

            @pl.when(jnp.logical_or(i != 0, c != cc))
            def _():
                gate_copy(i, cc).wait_send()

        for b in range(NX):

            @pl.when(jnp.logical_or(i != 0, x != b))
            def _():
                out_copy(b, i).wait_send()

    for j in range(2):
        for r in range(2):

            @pl.when(away(j, r))
            def _():
                log_copy(j, r).wait_send()

    for dz in range(1, NZ):
        z_logs(dz).wait_send()

    def drain(t, carry):
        d, p = t // 4 + 1, t % 4
        for way, hop in ((0, z_up), (1, z_down)):
            src = origin(way, d - 1)

            @pl.when(jnp.logical_and(src >= 0, goes(way, src, p, d)))
            def _():
                hop(src, p, t).wait_send()

            o = origin(way, d)

            @pl.when(jnp.logical_and(arrives(way, t), o < z))
            def _():
                z_pair(o, p, way, t).wait_send()

        return carry

    lax.fori_loop(0, 16, drain, 0)


def body(tokens, query_weight, key_weight, value_weight, gate_weight, forget_weight, forget_bias, out_weight):
    dma = pltpu.SemaphoreType.DMA
    vmem = pltpu.VMEM
    anywhere = pl.BlockSpec(memory_space=pl.ANY)
    local = pl.BlockSpec(memory_space=pltpu.VMEM)
    return pl.pallas_call(
        kernel,
        out_shape=jax.ShapeDtypeStruct((ROW, D), BF16),
        in_specs=[anywhere] * 5 + [local, local, anywhere],
        out_specs=local,
        scratch_shapes=[
            vmem((NY, SUB, D), BF16),
            vmem((D, WIDTH), BF16),
            vmem((D, WIDTH), BF16),
            vmem((D, WIDTH), BF16),
            vmem((D, WIDTH), BF16),
            vmem((D, D), BF16),
            vmem((NY, 2, 2, SUB, HD), BF16),
            vmem((NY, 2, SUB, HD), BF16),
            vmem((NY, SUB, WIDTH), F32),
            vmem((8, ROW, WIDTH), F32),
            vmem((8, 512), F32),
            vmem((2, 1, 512), F32),
            vmem((NZ * NX, 1, 512), F32),
            vmem((NZ, NY, 1, 512), F32),
            vmem((NZ, NY, 2, NX, SUB, HD), BF16),
            vmem((NX, NY, ROW, HD), BF16),
            vmem((NX, 256, HD), F32),
            vmem((NX, 256, HD), F32),
            vmem((NX, 256, HD), F32),
            vmem((NX, NY, ROW, HD), BF16),
            vmem((16, ROW, HD), BF16),
            vmem((ROW, D), BF16),
            dma((6,)),
            dma((2, 2)), dma((2, 2)), dma((2,)), dma((2,)), dma((4,)), dma((4,)),
            dma((4, 2, 2)), dma((4, 4)), dma((4, 2, 2)), dma((4, 4)),
            dma((4, 2)), dma((8,)),
            dma((2, 2)), dma((4,)), dma((8,)), dma((8,)),
            dma((4, 4)), dma((16,)),
            dma((2, 16)), dma((2, 16)), dma((2, 16)), dma((2, 16)), dma((4,)), dma((4,)),
        ],
        compiler_params=pltpu.CompilerParams(
            collective_id=0, has_side_effects=True, vmem_limit_bytes=60 * 1024 * 1024
        ),
    )(
        tokens, query_weight, key_weight, value_weight, gate_weight,
        forget_weight.T, forget_bias.reshape(1, 16), out_weight,
    )


def solution(mesh):
    placed = (
        P(("sp", "tp"), None), P(None, "tp"), P(None, "tp"), P(None, "tp"), P(None, "tp"), P(), P(), P(),
    )
    return jax.shard_map(
        body, mesh=mesh, in_specs=placed, out_specs=P(("sp", "tp"), None), check_vma=False
    )
```

```python
import jax
import jax.numpy as jnp
from jax import lax
from jax.experimental import pallas as pl
from jax.experimental.pallas import tpu as pltpu
from jax.sharding import PartitionSpec as P

NZ, NX, NY = 8, 4, 4
HD = 128
WIDTH = 256
D = 2048
SUB = 128
ROW = 64
HALF = 32
PARTS = (
    ((0, 0, ROW, 0),),
    ((NY - 1, 0, HALF, 0), (1, HALF, HALF, HALF)),
    ((NY - 1, 0, HALF, HALF), (1, HALF, HALF, 0)),
    ((2, 0, ROW, 0),),
)
MESH = pl.DeviceIdType.MESH
NT = (((1,), (1,)), ((), ()))
F32, BF16 = jnp.float32, jnp.bfloat16
LOG2E = 1.4426950408889634


def rcopy(src, dst, send, recv, sp, tp):
    return pltpu.make_async_remote_copy(
        src_ref=src,
        dst_ref=dst,
        send_sem=send,
        recv_sem=recv,
        device_id=(sp, tp),
        device_id_type=MESH,
    )


def kernel(
    tok_hbm, wq_hbm, wk_hbm, wv_hbm, wg_hbm, fw_hbm, fb_hbm, wo_hbm, out_ref,
    tok, wq, wk, wv, wg, fw_ref, fb_ref, wo, kvs, qs, gbuf, ggot, lg, lcs, lcbuf, cu, kv, q, acc, mx, ln, ob, obuf, att, fout,
    loc_s, ty_s, ty_r, tr_s, tr_r, tp_s, tp_r,
    xk_s, xk_r, xq_s, xq_r, g_s, g_r, l_s, l_r, lz_s, lz_r, o_s, o_r,
    zs, zr, ps, pr, po_s, po_r,
):
    sp = lax.axis_index("sp")
    tp = lax.axis_index("tp")
    z, x = sp // NX, sp % NX
    y, c = tp // 2, tp % 2
    other = y * 2 + (1 - c)
    up = ((z + 1) % NZ) * NX + x
    down = ((z + NZ - 1) % NZ) * NX + x
    ynext = ((y + 1) % NY) * 2 + c
    yprev = ((y + NY - 1) % NY) * 2 + c
    mine = pl.ds(pl.multiple_of(c * ROW, ROW), ROW)

    barrier = pltpu.get_barrier_semaphore()

    def greet(who_sp, who_tp):
        pl.semaphore_signal(barrier, inc=1, device_id=(who_sp, who_tp), device_id_type=MESH)

    greet(sp, other)
    for dy in range(1, NY):
        for core in range(2):
            greet(sp, ((y + dy) % NY) * 2 + core)
    for dz in range(1, NZ):
        greet(((z + dz) % NZ) * NX + x, tp)
    for dx in range(1, NX):
        xx = z * NX + (x + dx) % NX
        for core in range(2):
            greet(xx, y * 2 + core)
        for dy in range(1, NY):
            greet(xx, ((y + dy) % NY) * 2 + c)

    tok_cp = pltpu.make_async_copy(tok_hbm, tok.at[0, mine], loc_s.at[0])
    tok_cp.start()
    loads = [
        pltpu.make_async_copy(src, dst, loc_s.at[1 + n])
        for n, (src, dst) in enumerate(
            ((wk_hbm, wk), (wv_hbm, wv), (wq_hbm, wq), (wg_hbm, wg), (fw_hbm, fw_ref), (fb_hbm, fb_ref), (wo_hbm, wo))
        )
    ]
    for cp in loads[:6]:
        cp.start()

    tok_cp.wait()
    pl.semaphore_wait(barrier, 2 * NY - 1 + NZ - 1 + (NX - 1) * (NY + 1))

    def rows32(first):
        return pl.ds(pl.multiple_of(c * ROW + first, HALF), HALF)

    def tok_up(h):
        return rcopy(
            tok.at[0, rows32(h * HALF)], tok.at[1 + h, rows32(0)], ty_s.at[0, h], ty_r.at[0, h], sp, ynext
        )

    def tok_down(h):
        return rcopy(
            tok.at[0, rows32(h * HALF)], tok.at[2 - h, rows32(HALF)], ty_s.at[1, h], ty_r.at[1, h], sp, yprev
        )

    def relay_up():
        return rcopy(tok.at[1, rows32(0)], tok.at[3, rows32(0)], tr_s.at[0], tr_r.at[0], sp, ynext)

    def relay_down():
        return rcopy(tok.at[1, rows32(HALF)], tok.at[3, rows32(HALF)], tr_s.at[1], tr_r.at[1], sp, yprev)

    def tok_pair(i):
        return rcopy(tok.at[i, mine], tok.at[i, mine], tp_s.at[i], tp_r.at[i], sp, other)

    def wait_pair(i):
        theirs = pl.ds(pl.multiple_of((1 - c) * ROW, ROW), ROW)
        rcopy(tok.at[i, theirs], tok.at[i, theirs], tp_s.at[i], tp_r.at[i], sp, other).wait_recv()

    tok_up(0).start()
    tok_down(1).start()
    tok_pair(0).start()
    tok_up(1).start()
    tok_down(0).start()

    mx[...] = jnp.full_like(mx, -1e30)
    ln[...] = jnp.zeros_like(ln)
    acc[...] = jnp.zeros_like(acc)

    own_head = x // 2 == c
    own_j = x - 2 * c

    def x_kv(i, j, r):
        rows = pl.ds(r * ROW, ROW)
        return rcopy(
            kvs.at[i, j, :, rows], kv.at[z, i, :, x, rows], xk_s.at[i, j, r], xk_r.at[i, x],
            z * NX + 2 * c + j, y * 2 + r,
        )

    def x_q(i, j, r):
        rows = pl.ds(r * ROW, ROW)
        return rcopy(
            qs.at[i, j, rows], q.at[x, i], xq_s.at[i, j, r], xq_r.at[i, x],
            z * NX + 2 * c + j, y * 2 + r,
        )

    def gate_copy(i, n, cc):
        step, first, rows, into = PARTS[i][n]
        return rcopy(
            gbuf.at[i, pl.ds(cc * ROW + first, rows)], ggot.at[tp, pl.ds(into, rows)],
            g_s.at[i, n, cc], g_r.at[tp, into // HALF], sp, ((y + step) % NY) * 2 + cc,
        )

    def away(j, r):
        return jnp.logical_or(x != 2 * c + j, c != r)

    def project(i):
        part = tok[i]
        k = jnp.dot(part, wk[...], preferred_element_type=F32).astype(BF16)
        v = jnp.dot(part, wv[...], preferred_element_type=F32).astype(BF16)
        for j in range(2):
            kvs[i, j, 0] = k[:, j * HD : (j + 1) * HD]
            kvs[i, j, 1] = v[:, j * HD : (j + 1) * HD]
        for j in range(2):
            for r in range(2):

                @pl.when(away(j, r))
                def _():
                    x_kv(i, j, r).start()

        qq = (jnp.dot(part, wq[...], preferred_element_type=F32) * HD ** (-0.5)).astype(BF16)
        for j in range(2):
            qs[i, j] = qq[:, j * HD : (j + 1) * HD]
        for j in range(2):
            for r in range(2):

                @pl.when(away(j, r))
                def _():
                    x_q(i, j, r).start()

        for j in range(2):

            @pl.when(x == 2 * c + j)
            def _():
                kv[z, i, :, x, mine] = kvs[i, j, :, mine]
                q[x, i] = qs[i, j, mine]

        gate = jax.nn.sigmoid(jnp.dot(part, wg[...], preferred_element_type=F32))
        gbuf[i] = gate
        for cc in range(2):
            if i == 0:

                @pl.when(c != cc)
                def _():
                    gate_copy(i, 0, cc).start()

                @pl.when(c == cc)
                def _():
                    ggot[tp] = gbuf[i, cc * ROW : (cc + 1) * ROW]
            else:
                for n in range(len(PARTS[i])):
                    gate_copy(i, n, cc).start()
        diag = lax.broadcasted_iota(jnp.int32, (16, 16), 0) == lax.broadcasted_iota(jnp.int32, (16, 16), 1)
        bias = jnp.sum(jnp.where(diag, fb_ref[...], 0.0), axis=1, keepdims=True)
        logits = lax.dot_general(fw_ref[...], part, NT, preferred_element_type=F32) + bias
        small = jnp.exp(-jnp.abs(logits))
        grown = 1.0 + small
        tail = jnp.where(grown == 1.0, small, jnp.log(grown) * (small / jnp.where(grown == 1.0, 1.0, grown - 1.0)))
        logs = jnp.minimum(logits, 0.0) - tail
        pick = (
            lax.broadcasted_iota(jnp.int32, (8, 16), 1)
            == lax.broadcasted_iota(jnp.int32, (8, 16), 0) + 2 * tp
        ).astype(F32)
        turned = jnp.dot(pick, logs, precision=lax.Precision.HIGHEST, preferred_element_type=F32)
        lg[i] = turned

    def z_up(o, p, t):
        ref = kv.at[o, p, :, :, mine]
        return rcopy(ref, ref, zs.at[0, t], zr.at[0, t], up, tp)

    def z_down(o, p, t):
        ref = kv.at[o, p, :, :, mine]
        return rcopy(ref, ref, zs.at[1, t], zr.at[1, t], down, tp)

    def z_pair(o, p, way, t):
        ref = kv.at[o, p, :, :, mine]
        return rcopy(ref, ref, ps.at[way, t], pr.at[way, t], sp, other)

    def own_pair(p):
        ref = kv.at[z, p, :, :, mine]
        return rcopy(ref, ref, po_s.at[p], po_r.at[p], sp, other)

    def reach(way, p):
        return 3 + (p < 2).astype(jnp.int32) if way == 0 else 3 + (p >= 2).astype(jnp.int32)

    def goes(way, o, p, d):
        far = reach(way, p)
        if way == 0:
            return jnp.logical_and(d <= far, o + d < NZ)
        return jnp.logical_and(d <= far, o + 1 <= far)

    def first_sends(p):
        for xs in range(NX):

            @pl.when(jnp.logical_not(jnp.logical_and(own_head, x == xs)))
            def _():
                ref = kv.at[z, p, :, xs, mine]
                rcopy(ref, ref, xk_s.at[p, 0, 0], xk_r.at[p, xs], sp, other).wait_recv()

        pv = jnp.int32(p)

        @pl.when(goes(0, z, pv, 1))
        def _():
            z_up(z, p, p).start()

        @pl.when(goes(1, z, pv, 1))
        def _():
            z_down(z, p, p).start()

        own_pair(p).start()

    def origin(way, d):
        return z - d if way == 0 else (z + d) % NZ

    def piece(way, t):
        return t % 4 + (2 * (t >= 12).astype(jnp.int32) if way == 1 else 0)

    def arrives(way, t):
        o = origin(way, t // 4 + 1)
        return jnp.logical_and(o >= 0, goes(way, o, piece(way, t), t // 4 + 1))

    def relay(t):
        d = t // 4 + 1
        for way, hop in ((0, z_up), (1, z_down)):
            o, p = origin(way, d), piece(way, t)

            @pl.when(arrives(way, t))
            def _():
                hop(o, p, t).wait_recv()

                @pl.when(goes(way, o, p, d + 1))
                def _():
                    hop(o, p, t + 4 - (2 * (t >= 8).astype(jnp.int32) if way == 1 else 0)).start()

                @pl.when(o < z)
                def _():
                    z_pair(o, p, way, t).start()

    for cp in loads[:6]:
        cp.wait()
    wait_pair(0)
    project(0)
    loads[6].start()
    tok_up(0).wait_recv()
    relay_up().start()
    tok_down(1).wait_recv()
    relay_down().start()
    tok_pair(1).start()
    first_sends(0)
    wait_pair(1)
    project(1)
    tok_up(1).wait_recv()
    tok_down(0).wait_recv()
    tok_pair(2).start()
    first_sends(1)
    wait_pair(2)
    project(2)
    relay_up().wait_recv()
    relay_down().wait_recv()
    tok_pair(3).start()
    first_sends(2)
    relay(jnp.int32(0))
    relay(jnp.int32(1))
    wait_pair(3)
    project(3)

    even = (lax.broadcasted_iota(jnp.int32, (8, SUB), 1) // HALF) % 2 == 0
    before = jnp.where(even, lg[1], pltpu.roll(lg[2], HALF, 1))
    after = jnp.where(even, pltpu.roll(lg[2], SUB - HALF, 1), lg[1])
    tri = (
        lax.broadcasted_iota(jnp.int32, (SUB, SUB), 0) <= lax.broadcasted_iota(jnp.int32, (SUB, SUB), 1)
    ).astype(F32)
    chips = [lg[0], after, lg[3], before]
    sums = jnp.dot(
        jnp.concatenate(chips, axis=0), tri, precision=lax.Precision.HIGHEST, preferred_element_type=F32
    )
    sums = [sums[n * 8 : (n + 1) * 8] for n in range(NY)]
    totals = [part[:, SUB - 1 : SUB] for part in sums]
    moved = []
    for n in range(NY):
        past = jnp.zeros((8, 1), F32)
        for m in range(NY):
            past = past + jnp.where((y + m) % NY < (y + n) % NY, totals[m], 0.0)
        moved.append(sums[n] + past)
    own, after, far, before = moved
    in_order = (
        own,
        jnp.where(even, before, after),
        jnp.where(even, pltpu.roll(before, SUB - HALF, 1), pltpu.roll(after, HALF, 1)),
        far,
        jnp.broadcast_to((totals[0] + totals[1]) + (totals[2] + totals[3]), (8, SUB)),
    )
    for n, part in enumerate(in_order):
        for j in range(2):
            lcs[j, :, n * SUB : (n + 1) * SUB] = part[j : j + 1]

    def log_copy(j, r):
        return rcopy(lcs.at[j], lcbuf.at[sp], l_s.at[j, r], l_r.at[x], z * NX + 2 * c + j, y * 2 + r)

    for j in range(2):
        for r in range(2):

            @pl.when(away(j, r))
            def _():
                log_copy(j, r).start()

        @pl.when(x == 2 * c + j)
        def _():
            lcbuf[sp] = lcs[j]

    first_sends(3)

    def place(p, row):
        side = (row & HALF) >> 5
        steps = jnp.where(p == 0, 0, jnp.where(p == 3, 2, 3 + 2 * side))
        return ((y + steps) & 3) * SUB + (row ^ jnp.where(p == 2, HALF, 0))

    def attend(pieces, diagonal=False):
        rows = q[...].reshape(NX * 256, HD)
        scores = [
            lax.dot_general(rows, kv[o, p, 0].reshape(NX * SUB, HD), NT, preferred_element_type=F32)
            for o, p in pieces
        ]
        biases = [cu[o, p] for o, p in pieces]
        rounded, factors = [], []
        for b in range(NX):
            parts = []
            for score, bias in zip(scores, biases):
                s = score[b * 256 : (b + 1) * 256] * LOG2E - bias
                if diagonal:
                    row = lax.broadcasted_iota(jnp.int32, (256, 1), 0)
                    at_q = b * 512 + place(row >> 6, c * ROW + (row & 63))
                    lane = lax.broadcasted_iota(jnp.int32, (1, NX * SUB), 1)
                    at_k = (lane >> 7) * 512 + place(pieces[0][1], lane & 127)
                    s = jnp.where(at_k <= at_q, s, -jnp.inf)
                parts.append(s)
            old = mx[b]
            new = old
            for s in parts:
                new = jnp.maximum(new, jnp.max(s, axis=1, keepdims=True))
            factor = jnp.exp2(old - new)
            weights = [jnp.exp2(s[:, n * 128 : (n + 1) * 128] - new) for s in parts for n in range(NX)]
            sums = weights
            while len(sums) > 1:
                sums = [sums[n] + sums[n + 1] for n in range(0, len(sums), 2)]
            ln[b] = ln[b] * factor + sums[0]
            rounded.append(jnp.concatenate([w.astype(BF16) for w in weights], axis=1))
            factors.append(factor)
            mx[b] = new
        values = [kv[o, p, 1].reshape(NX * SUB, HD) for o, p in pieces]
        values = values[0] if len(values) == 1 else jnp.concatenate(values, axis=0)
        more = jnp.dot(jnp.concatenate(rounded, axis=0), values, preferred_element_type=F32)
        for b in range(NX):
            acc[b] = acc[b] * factors[b] + more[b * 256 : (b + 1) * 256]

    for xs in range(NX):

        @pl.when(jnp.logical_not(jnp.logical_and(own_head, x == xs)))
        def _():
            ref = lcbuf.at[z * NX + xs]
            rcopy(ref, ref, l_s.at[0, 0], l_r.at[xs], sp, other).wait_recv()

    def z_logs(dz):
        ref = lcbuf.at[pl.ds(z * NX, NX)]
        return rcopy(ref, ref, lz_s.at[dz], lz_r.at[z], ((z + dz) % NZ) * NX + x, tp)

    for dz in range(1, NZ):
        z_logs(dz).start()

    offset = jnp.zeros((1, 1), F32)
    for n in range(NX):
        line = lcbuf[z * NX + n]
        scaled = (line + offset) * LOG2E
        for i in range(NY):
            cu[z, i, :, n * SUB : (n + 1) * SUB] = scaled[:, i * SUB : (i + 1) * SUB]
        offset = offset + line[:, 512:513]

    for i in range(NY):
        for xs in range(NX):

            @pl.when(jnp.logical_not(jnp.logical_and(own_head, x == xs)))
            def _():
                ref = q.at[xs, i]
                rcopy(ref, ref, xq_s.at[i, 0, 0], xq_r.at[i, xs], sp, other).wait_recv()

    theirs = pl.ds(pl.multiple_of((1 - c) * ROW, ROW), ROW)

    def pair_wait(o, p, sem):
        ref = kv.at[o, p, :, :, theirs]
        rcopy(ref, ref, po_s.at[0], sem, sp, other).wait_recv()

    def consume(t):
        d = t // 4 + 1
        ups = arrives(0, t)
        o_up, o_down = origin(0, d), origin(1, d)
        p_up, p_down = piece(0, t), piece(1, t)
        downs = jnp.logical_and(arrives(1, t), o_down < z)

        @pl.when(ups)
        def _():
            pair_wait(o_up, p_up, pr.at[0, t])

        @pl.when(downs)
        def _():
            pair_wait(o_down, p_down, pr.at[1, t])

        @pl.when(jnp.logical_and(ups, downs))
        def _():
            attend([(o_up, p_up), (o_down, p_down)])

        @pl.when(jnp.logical_xor(ups, downs))
        def _():
            attend([(jnp.where(ups, o_up, o_down), jnp.where(ups, p_up, p_down))])

    def own_piece(t, carry):
        @pl.when(t >= 2)
        def _():
            relay(t)

        pair_wait(z, t, po_r.at[t])
        attend([(z, t)], diagonal=True)
        return carry

    lax.fori_loop(0, 4, own_piece, 0)

    for n in range(NZ):

        @pl.when(z != n)
        def _():
            ref = lcbuf.at[pl.ds(n * NX, NX)]
            rcopy(ref, ref, lz_s.at[1], lz_r.at[n], sp, other).wait_recv()

    base = jnp.zeros((1, 1), F32)
    for n in range(NZ * NX):
        base = base + jnp.where(n < NX * z, lcbuf[n, :, 512:513], 0.0)
    offset = -base
    for n in range(NZ * NX):
        line = lcbuf[n]
        scaled = (line + offset) * LOG2E
        for i in range(NY):
            cu[n // NX, i, :, (n % NX) * SUB : (n % NX + 1) * SUB] = scaled[:, i * SUB : (i + 1) * SUB]
        offset = offset + line[:, 512:513]

    def step(t, carry):
        @pl.when(jnp.logical_and(t >= 3, t < 13))
        def _():
            relay(t + 1)

        consume(t)
        return carry

    lax.fori_loop(0, 14, step, 0)

    head = y * NX + x

    def out_copy(b, i, n):
        ahead, first, rows, into = PARTS[i][n]
        return rcopy(
            ob.at[b, i, pl.ds(first, rows)], obuf.at[head, pl.ds(into, rows)],
            o_s.at[b, i, n], o_r.at[head, into // HALF], z * NX + b, ((y + ahead) % NY) * 2 + c,
        )

    for b in range(NX):
        done = acc[b] / jnp.sum(ln[b], axis=1, keepdims=True)
        ob[b] = done.astype(BF16).reshape(NY, ROW, HD)
        for i in (3, 1, 2, 0):
            if i == 0:

                @pl.when(x != b)
                def _():
                    out_copy(b, 0, 0).start()

                @pl.when(x == b)
                def _():
                    obuf[head] = ob[b, 0]
            else:
                for n in range(len(PARTS[i])):
                    out_copy(b, i, n).start()

    for h in range(2):
        tok_up(h).wait_send()
        tok_down(h).wait_send()
    relay_up().wait_send()
    relay_down().wait_send()
    for i in range(NY):
        tok_pair(i).wait_send()
        own_pair(i).wait_send()
        for j in range(2):
            for r in range(2):

                @pl.when(away(j, r))
                def _():
                    x_kv(i, j, r).wait_send()
                    x_q(i, j, r).wait_send()

        for cc in range(2):
            for n in range(len(PARTS[i])):

                @pl.when(jnp.logical_or(i != 0, c != cc))
                def _():
                    gate_copy(i, n, cc).wait_send()

    for j in range(2):
        for r in range(2):

            @pl.when(away(j, r))
            def _():
                log_copy(j, r).wait_send()

    for dz in range(1, NZ):
        z_logs(dz).wait_send()

    def drain(t, carry):
        d = t // 4 + 1
        for way, hop in ((0, z_up), (1, z_down)):
            p = piece(way, t)
            src = origin(way, d - 1)

            @pl.when(jnp.logical_and(src >= 0, goes(way, src, p, d)))
            def _():
                hop(src, p, t).wait_send()

            o = origin(way, d)

            @pl.when(jnp.logical_and(arrives(way, t), o < z))
            def _():
                z_pair(o, p, way, t).wait_send()

        return carry

    lax.fori_loop(0, 14, drain, 0)

    loads[6].wait()
    for ahead in (0, 1, 3, 2):
        yy = (y + ahead) % NY
        for core in range(2):
            who = yy * 2 + core
            for into in range(0, ROW, ROW if ahead % 2 == 0 else HALF):
                ref = ggot.at[who, pl.ds(into, ROW if ahead % 2 == 0 else HALF)]

                def got():
                    rcopy(ref, ref, g_s.at[0, 0, 0], g_r.at[who, into // HALF], sp, other).wait_recv()

                if ahead == 0:
                    pl.when(core != c)(got)
                else:
                    got()
        for xx in range(NX):
            h = yy * NX + xx
            for into in range(0, ROW, ROW if ahead % 2 == 0 else HALF):
                ref = obuf.at[h, pl.ds(into, ROW if ahead % 2 == 0 else HALF)]

                def came():
                    rcopy(ref, ref, o_s.at[0, 0, 0], o_r.at[h, into // HALF], sp, other).wait_recv()

                if ahead == 0:
                    pl.when(xx != x)(came)
                else:
                    came()
            gate = ggot[yy * 2 + xx // 2, :, xx % 2 * HD : (xx % 2 + 1) * HD]
            att[:, xx * HD : (xx + 1) * HD] = (obuf[h].astype(F32) * gate).astype(BF16)
        share = pl.ds(pl.multiple_of(yy * NX * HD, NX * HD), NX * HD)
        for n in range(4):
            cols = slice(n * 512, (n + 1) * 512)
            more = jnp.dot(att[...], wo[share, cols], preferred_element_type=F32)
            if ahead == 0:
                fout[:, cols] = more
            elif ahead != 2:
                fout[:, cols] += more
            else:
                out_ref[:, cols] = (fout[:, cols] + more).astype(BF16)

    for b in range(NX):
        for i in range(NY):
            for n in range(len(PARTS[i])):

                @pl.when(jnp.logical_or(i != 0, x != b))
                def _():
                    out_copy(b, i, n).wait_send()


def body(tokens, query_weight, key_weight, value_weight, gate_weight, forget_weight, forget_bias, out_weight):
    dma = pltpu.SemaphoreType.DMA
    vmem = pltpu.VMEM
    anywhere = pl.BlockSpec(memory_space=pl.ANY)
    local = pl.BlockSpec(memory_space=pltpu.VMEM)
    return pl.pallas_call(
        kernel,
        out_shape=jax.ShapeDtypeStruct((ROW, D), BF16),
        in_specs=[anywhere] * 8,
        out_specs=local,
        scratch_shapes=[
            vmem((NY, SUB, D), BF16),
            vmem((D, WIDTH), BF16),
            vmem((D, WIDTH), BF16),
            vmem((D, WIDTH), BF16),
            vmem((D, WIDTH), BF16),
            vmem((16, D), BF16),
            vmem((1, 16), F32),
            vmem((D, D), BF16),
            vmem((NY, 2, 2, SUB, HD), BF16),
            vmem((NY, 2, SUB, HD), BF16),
            vmem((NY, SUB, WIDTH), F32),
            vmem((8, ROW, WIDTH), F32),
            vmem((NY, 8, SUB), F32),
            vmem((2, 1, 640), F32),
            vmem((NZ * NX, 1, 640), F32),
            vmem((NZ, NY, 1, 512), F32),
            vmem((NZ, NY, 2, NX, SUB, HD), BF16),
            vmem((NX, NY, ROW, HD), BF16),
            vmem((NX, 256, HD), F32),
            vmem((NX, 256, HD), F32),
            vmem((NX, 256, HD), F32),
            vmem((NX, NY, ROW, HD), BF16),
            vmem((16, ROW, HD), BF16),
            vmem((ROW, NX * HD), BF16),
            vmem((ROW, D), F32),
            dma((8,)),
            dma((2, 2)), dma((2, 2)), dma((2,)), dma((2,)), dma((4,)), dma((4,)),
            dma((4, 2, 2)), dma((4, 4)), dma((4, 2, 2)), dma((4, 4)),
            dma((4, 2, 2)), dma((8, 2)),
            dma((2, 2)), dma((4,)), dma((8,)), dma((8,)),
            dma((4, 4, 2)), dma((16, 2)),
            dma((2, 16)), dma((2, 16)), dma((2, 16)), dma((2, 16)), dma((4,)), dma((4,)),
        ],
        compiler_params=pltpu.CompilerParams(
            collective_id=0, has_side_effects=True, vmem_limit_bytes=60 * 1024 * 1024
        ),
    )(
        tokens, query_weight, key_weight, value_weight, gate_weight,
        forget_weight.T, forget_bias.reshape(1, 16), out_weight,
    )


def solution(mesh):
    placed = (
        P(("sp", "tp"), None), P(None, "tp"), P(None, "tp"), P(None, "tp"), P(None, "tp"), P(), P(), P(),
    )
    return jax.shard_map(
        body, mesh=mesh, in_specs=placed, out_specs=P(("sp", "tp"), None), check_vma=False
    )
```

```python
import jax
import jax.numpy as jnp
from jax import lax
from jax.experimental import pallas as pl
from jax.experimental.pallas import tpu as pltpu
from jax.sharding import PartitionSpec as P

NZ, NX, NY = 8, 4, 4
HD = 128
WIDTH = 256
D = 2048
SUB = 128
ROW = 64
HALF = 32
PARTS = (
    ((0, 0, ROW, 0),),
    ((NY - 1, 0, HALF, 0), (1, HALF, HALF, HALF)),
    ((NY - 1, 0, HALF, HALF), (1, HALF, HALF, 0)),
    ((2, 0, ROW, 0),),
)
MESH = pl.DeviceIdType.MESH
NT = (((1,), (1,)), ((), ()))
F32, BF16 = jnp.float32, jnp.bfloat16
LOG2E = 1.4426950408889634


def rcopy(src, dst, send, recv, sp, tp):
    return pltpu.make_async_remote_copy(
        src_ref=src,
        dst_ref=dst,
        send_sem=send,
        recv_sem=recv,
        device_id=(sp, tp),
        device_id_type=MESH,
    )


def kernel(
    tok_hbm, wq_hbm, wk_hbm, wv_hbm, wg_hbm, fw_hbm, fb_hbm, wo_hbm, out_ref,
    tok, wq, wk, wv, wg, fw_ref, fb_ref, wo, kvs, qs, gbuf, ggot, lg, lcs, lcbuf, cu, kv, q, acc, mx, ln, ob, obuf, att, fout,
    loc_s, ty_s, ty_r, tr_s, tr_r, tp_s, tp_r,
    xk_s, xk_r, xq_s, xq_r, g_s, g_r, l_s, l_r, lz_s, lz_r, o_s, o_r,
    zs, zr, ps, pr, po_s, po_r,
):
    sp = lax.axis_index("sp")
    tp = lax.axis_index("tp")
    z, x = sp // NX, sp % NX
    y, c = tp // 2, tp % 2
    other = y * 2 + (1 - c)
    up = ((z + 1) % NZ) * NX + x
    down = ((z + NZ - 1) % NZ) * NX + x
    ynext = ((y + 1) % NY) * 2 + c
    yprev = ((y + NY - 1) % NY) * 2 + c
    mine = pl.ds(pl.multiple_of(c * ROW, ROW), ROW)

    barrier = pltpu.get_barrier_semaphore()

    def greet(who_sp, who_tp):
        pl.semaphore_signal(barrier, inc=1, device_id=(who_sp, who_tp), device_id_type=MESH)

    greet(sp, other)
    for dy in range(1, NY):
        for core in range(2):
            greet(sp, ((y + dy) % NY) * 2 + core)
    for dz in (1, 2, NZ - 1, NZ - 2):
        greet(((z + dz) % NZ) * NX + x, tp)
    for dx in range(1, NX):
        for core in range(2):
            greet(z * NX + (x + dx) % NX, y * 2 + core)

    tok_cp = pltpu.make_async_copy(tok_hbm, tok.at[0, mine], loc_s.at[0])
    tok_cp.start()
    loads = [
        pltpu.make_async_copy(src, dst, loc_s.at[1 + n])
        for n, (src, dst) in enumerate(
            ((wk_hbm, wk), (wv_hbm, wv), (wq_hbm, wq), (wg_hbm, wg), (fw_hbm, fw_ref), (fb_hbm, fb_ref), (wo_hbm, wo))
        )
    ]
    for cp in loads[:6]:
        cp.start()

    tok_cp.wait()
    pl.semaphore_wait(barrier, 2 * NY - 1 + 4 + (NX - 1) * 2)

    def rows32(first):
        return pl.ds(pl.multiple_of(c * ROW + first, HALF), HALF)

    def tok_up(h):
        return rcopy(
            tok.at[0, rows32(h * HALF)], tok.at[1 + h, rows32(0)], ty_s.at[0, h], ty_r.at[0, h], sp, ynext
        )

    def tok_down(h):
        return rcopy(
            tok.at[0, rows32(h * HALF)], tok.at[2 - h, rows32(HALF)], ty_s.at[1, h], ty_r.at[1, h], sp, yprev
        )

    def relay_up():
        return rcopy(tok.at[1, rows32(0)], tok.at[3, rows32(0)], tr_s.at[0], tr_r.at[0], sp, ynext)

    def relay_down():
        return rcopy(tok.at[1, rows32(HALF)], tok.at[3, rows32(HALF)], tr_s.at[1], tr_r.at[1], sp, yprev)

    def tok_pair(i):
        return rcopy(tok.at[i, mine], tok.at[i, mine], tp_s.at[i], tp_r.at[i], sp, other)

    def wait_pair(i):
        theirs = pl.ds(pl.multiple_of((1 - c) * ROW, ROW), ROW)
        rcopy(tok.at[i, theirs], tok.at[i, theirs], tp_s.at[i], tp_r.at[i], sp, other).wait_recv()

    tok_up(0).start()
    tok_down(1).start()
    tok_pair(0).start()
    tok_up(1).start()
    tok_down(0).start()

    mx[...] = jnp.full_like(mx, -1e30)
    ln[...] = jnp.zeros_like(ln)
    acc[...] = jnp.zeros_like(acc)

    own_head = x // 2 == c
    own_j = x - 2 * c

    def x_kv(i, j, r):
        rows = pl.ds(r * ROW, ROW)
        return rcopy(
            kvs.at[i, j, :, rows], kv.at[z, i, :, x, rows], xk_s.at[i, j, r], xk_r.at[i, x],
            z * NX + 2 * c + j, y * 2 + r,
        )

    def x_q(i, j, r):
        rows = pl.ds(r * ROW, ROW)
        return rcopy(
            qs.at[i, j, rows], q.at[x, i], xq_s.at[i, j, r], xq_r.at[i, x],
            z * NX + 2 * c + j, y * 2 + r,
        )

    def gate_copy(i, n, cc):
        step, first, rows, into = PARTS[i][n]
        return rcopy(
            gbuf.at[i, pl.ds(cc * ROW + first, rows)], ggot.at[tp, pl.ds(into, rows)],
            g_s.at[i, n, cc], g_r.at[tp, into // HALF], sp, ((y + step) % NY) * 2 + cc,
        )

    def away(j, r):
        return jnp.logical_or(x != 2 * c + j, c != r)

    def project(i):
        part = tok[i]
        k = jnp.dot(part, wk[...], preferred_element_type=F32).astype(BF16)
        v = jnp.dot(part, wv[...], preferred_element_type=F32).astype(BF16)
        for j in range(2):
            kvs[i, j, 0] = k[:, j * HD : (j + 1) * HD]
            kvs[i, j, 1] = v[:, j * HD : (j + 1) * HD]
        for j in range(2):
            for r in range(2):

                @pl.when(away(j, r))
                def _():
                    x_kv(i, j, r).start()

        qq = (jnp.dot(part, wq[...], preferred_element_type=F32) * HD ** (-0.5)).astype(BF16)
        for j in range(2):
            qs[i, j] = qq[:, j * HD : (j + 1) * HD]
        for j in range(2):
            for r in range(2):

                @pl.when(away(j, r))
                def _():
                    x_q(i, j, r).start()

        for j in range(2):

            @pl.when(x == 2 * c + j)
            def _():
                kv[z, i, :, x, mine] = kvs[i, j, :, mine]
                q[x, i] = qs[i, j, mine]

        gate = jax.nn.sigmoid(jnp.dot(part, wg[...], preferred_element_type=F32))
        gbuf[i] = gate
        for cc in range(2):
            if i == 0:

                @pl.when(c != cc)
                def _():
                    gate_copy(i, 0, cc).start()

                @pl.when(c == cc)
                def _():
                    ggot[tp] = gbuf[i, cc * ROW : (cc + 1) * ROW]
            else:
                for n in range(len(PARTS[i])):
                    gate_copy(i, n, cc).start()
        diag = lax.broadcasted_iota(jnp.int32, (16, 16), 0) == lax.broadcasted_iota(jnp.int32, (16, 16), 1)
        bias = jnp.sum(jnp.where(diag, fb_ref[...], 0.0), axis=1, keepdims=True)
        logits = lax.dot_general(fw_ref[...], part, NT, preferred_element_type=F32) + bias
        small = jnp.exp(-jnp.abs(logits))
        grown = 1.0 + small
        tail = jnp.where(grown == 1.0, small, jnp.log(grown) * (small / jnp.where(grown == 1.0, 1.0, grown - 1.0)))
        logs = jnp.minimum(logits, 0.0) - tail
        pick = (
            lax.broadcasted_iota(jnp.int32, (8, 16), 1)
            == lax.broadcasted_iota(jnp.int32, (8, 16), 0) + 2 * tp
        ).astype(F32)
        turned = jnp.dot(pick, logs, precision=lax.Precision.HIGHEST, preferred_element_type=F32)
        lg[i] = turned

    def z_up(o, p, t):
        ref = kv.at[o, p, :, :, mine]
        return rcopy(ref, ref, zs.at[0, t], zr.at[0, t], up, tp)

    def z_down(o, p, t):
        ref = kv.at[o, p, :, :, mine]
        return rcopy(ref, ref, zs.at[1, t], zr.at[1, t], down, tp)

    def z_pair(o, p, way, t):
        ref = kv.at[o, p, :, :, mine]
        return rcopy(ref, ref, ps.at[way, t], pr.at[way, t], sp, other)

    def own_pair(p):
        ref = kv.at[z, p, :, :, mine]
        return rcopy(ref, ref, po_s.at[p], po_r.at[p], sp, other)

    def reach(way, p):
        return 3 + (p < 2).astype(jnp.int32) if way == 0 else 3 + (p >= 2).astype(jnp.int32)

    def goes(way, o, p, d):
        far = reach(way, p)
        if way == 0:
            return jnp.logical_and(d <= far, o + d < NZ)
        return jnp.logical_and(d <= far, o + 1 <= far)

    def first_sends(p):
        for xs in range(NX):

            @pl.when(jnp.logical_not(jnp.logical_and(own_head, x == xs)))
            def _():
                ref = kv.at[z, p, :, xs, mine]
                rcopy(ref, ref, xk_s.at[p, 0, 0], xk_r.at[p, xs], sp, other).wait_recv()

        pv = jnp.int32(p)

        @pl.when(goes(0, z, pv, 1))
        def _():
            z_up(z, p, p).start()

        @pl.when(goes(1, z, pv, 1))
        def _():
            z_down(z, p, p).start()

        own_pair(p).start()

    def origin(way, d):
        return z - d if way == 0 else (z + d) % NZ

    def piece(way, t):
        return t % 4 + (2 * (t >= 12).astype(jnp.int32) if way == 1 else 0)

    def arrives(way, t):
        o = origin(way, t // 4 + 1)
        return jnp.logical_and(o >= 0, goes(way, o, piece(way, t), t // 4 + 1))

    def relay(t):
        d = t // 4 + 1
        for way, hop in ((0, z_up), (1, z_down)):
            o, p = origin(way, d), piece(way, t)

            @pl.when(arrives(way, t))
            def _():
                hop(o, p, t).wait_recv()

                @pl.when(goes(way, o, p, d + 1))
                def _():
                    hop(o, p, t + 4 - (2 * (t >= 8).astype(jnp.int32) if way == 1 else 0)).start()

                @pl.when(o < z)
                def _():
                    z_pair(o, p, way, t).start()

    for cp in loads[:6]:
        cp.wait()
    wait_pair(0)
    project(0)
    loads[6].start()
    tok_up(0).wait_recv()
    relay_up().start()
    tok_down(1).wait_recv()
    relay_down().start()
    tok_pair(1).start()
    first_sends(0)
    wait_pair(1)
    project(1)
    tok_up(1).wait_recv()
    tok_down(0).wait_recv()
    tok_pair(2).start()
    first_sends(1)
    wait_pair(2)
    project(2)
    relay(jnp.int32(0))
    relay_up().wait_recv()
    relay_down().wait_recv()
    tok_pair(3).start()
    first_sends(2)
    relay(jnp.int32(1))
    wait_pair(3)
    project(3)

    even = (lax.broadcasted_iota(jnp.int32, (8, SUB), 1) // HALF) % 2 == 0
    before = jnp.where(even, lg[1], pltpu.roll(lg[2], HALF, 1))
    after = jnp.where(even, pltpu.roll(lg[2], SUB - HALF, 1), lg[1])
    tri = (
        lax.broadcasted_iota(jnp.int32, (SUB, SUB), 0) <= lax.broadcasted_iota(jnp.int32, (SUB, SUB), 1)
    ).astype(F32)
    chips = [lg[0], after, lg[3], before]
    sums = jnp.dot(
        jnp.concatenate(chips, axis=0), tri, precision=lax.Precision.HIGHEST, preferred_element_type=F32
    )
    sums = [sums[n * 8 : (n + 1) * 8] for n in range(NY)]
    totals = [part[:, SUB - 1 : SUB] for part in sums]
    moved = []
    for n in range(NY):
        past = jnp.zeros((8, 1), F32)
        for m in range(NY):
            past = past + jnp.where((y + m) % NY < (y + n) % NY, totals[m], 0.0)
        moved.append(sums[n] + past)
    own, after, far, before = moved
    in_order = (
        own,
        jnp.where(even, before, after),
        jnp.where(even, pltpu.roll(before, SUB - HALF, 1), pltpu.roll(after, HALF, 1)),
        far,
        jnp.broadcast_to((totals[0] + totals[1]) + (totals[2] + totals[3]), (8, SUB)),
    )
    for n, part in enumerate(in_order):
        for j in range(2):
            lcs[j, :, n * SUB : (n + 1) * SUB] = part[j : j + 1]

    def log_copy(j, r):
        return rcopy(lcs.at[j], lcbuf.at[sp], l_s.at[j, r], l_r.at[x], z * NX + 2 * c + j, y * 2 + r)

    for j in range(2):
        for r in range(2):

            @pl.when(away(j, r))
            def _():
                log_copy(j, r).start()

        @pl.when(x == 2 * c + j)
        def _():
            lcbuf[sp] = lcs[j]

    first_sends(3)

    def place(p, row):
        side = (row & HALF) >> 5
        steps = jnp.where(p == 0, 0, jnp.where(p == 3, 2, 3 + 2 * side))
        return ((y + steps) & 3) * SUB + (row ^ jnp.where(p == 2, HALF, 0))

    def attend(pieces, diagonal=False):
        rows = q[...].reshape(NX * 256, HD)
        scores = [
            lax.dot_general(rows, kv[o, p, 0].reshape(NX * SUB, HD), NT, preferred_element_type=F32)
            for o, p in pieces
        ]
        biases = [cu[o, p] for o, p in pieces]
        rounded, factors = [], []
        for b in range(NX):
            parts = []
            for score, bias in zip(scores, biases):
                s = score[b * 256 : (b + 1) * 256] * LOG2E - bias
                if diagonal:
                    row = lax.broadcasted_iota(jnp.int32, (256, 1), 0)
                    at_q = b * 512 + place(row >> 6, c * ROW + (row & 63))
                    lane = lax.broadcasted_iota(jnp.int32, (1, NX * SUB), 1)
                    at_k = (lane >> 7) * 512 + place(pieces[0][1], lane & 127)
                    s = jnp.where(at_k <= at_q, s, -jnp.inf)
                parts.append(s)
            old = mx[b]
            new = old
            for s in parts:
                new = jnp.maximum(new, jnp.max(s, axis=1, keepdims=True))
            factor = jnp.exp2(old - new)
            weights = [jnp.exp2(s[:, n * 128 : (n + 1) * 128] - new) for s in parts for n in range(NX)]
            sums = weights
            while len(sums) > 1:
                sums = [sums[n] + sums[n + 1] for n in range(0, len(sums), 2)]
            ln[b] = ln[b] * factor + sums[0]
            rounded.append(jnp.concatenate([w.astype(BF16) for w in weights], axis=1))
            factors.append(factor)
            mx[b] = new
        values = [kv[o, p, 1].reshape(NX * SUB, HD) for o, p in pieces]
        values = values[0] if len(values) == 1 else jnp.concatenate(values, axis=0)
        more = jnp.dot(jnp.concatenate(rounded, axis=0), values, preferred_element_type=F32)
        for b in range(NX):
            acc[b] = acc[b] * factors[b] + more[b * 256 : (b + 1) * 256]

    for xs in range(NX):

        @pl.when(jnp.logical_not(jnp.logical_and(own_head, x == xs)))
        def _():
            ref = lcbuf.at[z * NX + xs]
            rcopy(ref, ref, l_s.at[0, 0], l_r.at[xs], sp, other).wait_recv()

    HOPS = ((0, 1), (0, 2), (0, NZ - 1), (0, NZ - 2), (NZ - 1, 2), (NZ - 2, 2), (1, NZ - 2))

    def z_logs(n):
        whose, dz = HOPS[n]
        block = (z + whose) % NZ
        ref = lcbuf.at[pl.ds(block * NX, NX)]
        return rcopy(ref, ref, lz_s.at[n], lz_r.at[block], ((z + dz) % NZ) * NX + x, tp)

    def z_logs_wait(back):
        block = (z + NZ - back) % NZ
        ref = lcbuf.at[pl.ds(block * NX, NX)]
        rcopy(ref, ref, lz_s.at[0], lz_r.at[block], sp, other).wait_recv()

    for n in range(4):
        z_logs(n).start()

    offset = jnp.zeros((1, 1), F32)
    for n in range(NX):
        line = lcbuf[z * NX + n]
        scaled = (line + offset) * LOG2E
        for i in range(NY):
            cu[z, i, :, n * SUB : (n + 1) * SUB] = scaled[:, i * SUB : (i + 1) * SUB]
        offset = offset + line[:, 512:513]

    for i in range(NY):
        for xs in range(NX):

            @pl.when(jnp.logical_not(jnp.logical_and(own_head, x == xs)))
            def _():
                ref = q.at[xs, i]
                rcopy(ref, ref, xq_s.at[i, 0, 0], xq_r.at[i, xs], sp, other).wait_recv()

    theirs = pl.ds(pl.multiple_of((1 - c) * ROW, ROW), ROW)

    def pair_wait(o, p, sem):
        ref = kv.at[o, p, :, :, theirs]
        rcopy(ref, ref, po_s.at[0], sem, sp, other).wait_recv()

    def consume(t):
        d = t // 4 + 1
        ups = arrives(0, t)
        o_up, o_down = origin(0, d), origin(1, d)
        p_up, p_down = piece(0, t), piece(1, t)
        downs = jnp.logical_and(arrives(1, t), o_down < z)

        @pl.when(ups)
        def _():
            pair_wait(o_up, p_up, pr.at[0, t])

        @pl.when(downs)
        def _():
            pair_wait(o_down, p_down, pr.at[1, t])

        @pl.when(jnp.logical_and(ups, downs))
        def _():
            attend([(o_up, p_up), (o_down, p_down)])

        @pl.when(jnp.logical_xor(ups, downs))
        def _():
            attend([(jnp.where(ups, o_up, o_down), jnp.where(ups, p_up, p_down))])

    def own_piece(t, carry):
        @pl.when(t >= 2)
        def _():
            relay(t)

        pair_wait(z, t, po_r.at[t])
        attend([(z, t)], diagonal=True)
        return carry

    lax.fori_loop(0, 2, own_piece, 0)
    for back in (1, 2, NZ - 1):
        z_logs_wait(back)
    for n in range(4, 7):
        z_logs(n).start()
    lax.fori_loop(2, 4, own_piece, 0)
    for back in (3, 4, 5, 6):
        z_logs_wait(back)

    base = jnp.zeros((1, 1), F32)
    for n in range(NZ * NX):
        base = base + jnp.where(n < NX * z, lcbuf[n, :, 512:513], 0.0)
    offset = -base
    for n in range(NZ * NX):
        line = lcbuf[n]
        scaled = (line + offset) * LOG2E
        for i in range(NY):
            cu[n // NX, i, :, (n % NX) * SUB : (n % NX + 1) * SUB] = scaled[:, i * SUB : (i + 1) * SUB]
        offset = offset + line[:, 512:513]

    def step(t, carry):
        @pl.when(jnp.logical_and(t >= 3, t < 13))
        def _():
            relay(t + 1)

        consume(t)
        return carry

    lax.fori_loop(0, 14, step, 0)

    head = y * NX + x

    def out_copy(b, i, n):
        ahead, first, rows, into = PARTS[i][n]
        return rcopy(
            ob.at[b, i, pl.ds(first, rows)], obuf.at[head, pl.ds(into, rows)],
            o_s.at[b, i, n], o_r.at[head, into // HALF], z * NX + b, ((y + ahead) % NY) * 2 + c,
        )

    for b in range(NX):
        done = acc[b] / jnp.sum(ln[b], axis=1, keepdims=True)
        ob[b] = done.astype(BF16).reshape(NY, ROW, HD)
        for i in (3, 1, 2, 0):
            if i == 0:

                @pl.when(x != b)
                def _():
                    out_copy(b, 0, 0).start()

                @pl.when(x == b)
                def _():
                    obuf[head] = ob[b, 0]
            else:
                for n in range(len(PARTS[i])):
                    out_copy(b, i, n).start()

    for h in range(2):
        tok_up(h).wait_send()
        tok_down(h).wait_send()
    relay_up().wait_send()
    relay_down().wait_send()
    for i in range(NY):
        tok_pair(i).wait_send()
        own_pair(i).wait_send()
        for j in range(2):
            for r in range(2):

                @pl.when(away(j, r))
                def _():
                    x_kv(i, j, r).wait_send()
                    x_q(i, j, r).wait_send()

        for cc in range(2):
            for n in range(len(PARTS[i])):

                @pl.when(jnp.logical_or(i != 0, c != cc))
                def _():
                    gate_copy(i, n, cc).wait_send()

    for j in range(2):
        for r in range(2):

            @pl.when(away(j, r))
            def _():
                log_copy(j, r).wait_send()

    for n in range(7):
        z_logs(n).wait_send()

    def drain(t, carry):
        d = t // 4 + 1
        for way, hop in ((0, z_up), (1, z_down)):
            p = piece(way, t)
            src = origin(way, d - 1)

            @pl.when(jnp.logical_and(src >= 0, goes(way, src, p, d)))
            def _():
                hop(src, p, t).wait_send()

            o = origin(way, d)

            @pl.when(jnp.logical_and(arrives(way, t), o < z))
            def _():
                z_pair(o, p, way, t).wait_send()

        return carry

    lax.fori_loop(0, 14, drain, 0)

    loads[6].wait()
    for ahead in (0, 1, 3, 2):
        yy = (y + ahead) % NY
        for core in range(2):
            who = yy * 2 + core
            for into in range(0, ROW, ROW if ahead % 2 == 0 else HALF):
                ref = ggot.at[who, pl.ds(into, ROW if ahead % 2 == 0 else HALF)]

                def got():
                    rcopy(ref, ref, g_s.at[0, 0, 0], g_r.at[who, into // HALF], sp, other).wait_recv()

                if ahead == 0:
                    pl.when(core != c)(got)
                else:
                    got()
        for xx in range(NX):
            h = yy * NX + xx
            for into in range(0, ROW, ROW if ahead % 2 == 0 else HALF):
                ref = obuf.at[h, pl.ds(into, ROW if ahead % 2 == 0 else HALF)]

                def came():
                    rcopy(ref, ref, o_s.at[0, 0, 0], o_r.at[h, into // HALF], sp, other).wait_recv()

                if ahead == 0:
                    pl.when(xx != x)(came)
                else:
                    came()
            gate = ggot[yy * 2 + xx // 2, :, xx % 2 * HD : (xx % 2 + 1) * HD]
            att[:, xx * HD : (xx + 1) * HD] = (obuf[h].astype(F32) * gate).astype(BF16)
        share = pl.ds(pl.multiple_of(yy * NX * HD, NX * HD), NX * HD)
        for n in range(4):
            cols = slice(n * 512, (n + 1) * 512)
            more = jnp.dot(att[...], wo[share, cols], preferred_element_type=F32)
            if ahead == 0:
                fout[:, cols] = more
            elif ahead != 2:
                fout[:, cols] += more
            else:
                out_ref[:, cols] = (fout[:, cols] + more).astype(BF16)

    for b in range(NX):
        for i in range(NY):
            for n in range(len(PARTS[i])):

                @pl.when(jnp.logical_or(i != 0, x != b))
                def _():
                    out_copy(b, i, n).wait_send()


def body(tokens, query_weight, key_weight, value_weight, gate_weight, forget_weight, forget_bias, out_weight):
    dma = pltpu.SemaphoreType.DMA
    vmem = pltpu.VMEM
    anywhere = pl.BlockSpec(memory_space=pl.ANY)
    local = pl.BlockSpec(memory_space=pltpu.VMEM)
    return pl.pallas_call(
        kernel,
        out_shape=jax.ShapeDtypeStruct((ROW, D), BF16),
        in_specs=[anywhere] * 8,
        out_specs=local,
        scratch_shapes=[
            vmem((NY, SUB, D), BF16),
            vmem((D, WIDTH), BF16),
            vmem((D, WIDTH), BF16),
            vmem((D, WIDTH), BF16),
            vmem((D, WIDTH), BF16),
            vmem((16, D), BF16),
            vmem((1, 16), F32),
            vmem((D, D), BF16),
            vmem((NY, 2, 2, SUB, HD), BF16),
            vmem((NY, 2, SUB, HD), BF16),
            vmem((NY, SUB, WIDTH), F32),
            vmem((8, ROW, WIDTH), F32),
            vmem((NY, 8, SUB), F32),
            vmem((2, 1, 640), F32),
            vmem((NZ * NX, 1, 640), F32),
            vmem((NZ, NY, 1, 512), F32),
            vmem((NZ, NY, 2, NX, SUB, HD), BF16),
            vmem((NX, NY, ROW, HD), BF16),
            vmem((NX, 256, HD), F32),
            vmem((NX, 256, HD), F32),
            vmem((NX, 256, HD), F32),
            vmem((NX, NY, ROW, HD), BF16),
            vmem((16, ROW, HD), BF16),
            vmem((ROW, NX * HD), BF16),
            vmem((ROW, D), F32),
            dma((8,)),
            dma((2, 2)), dma((2, 2)), dma((2,)), dma((2,)), dma((4,)), dma((4,)),
            dma((4, 2, 2)), dma((4, 4)), dma((4, 2, 2)), dma((4, 4)),
            dma((4, 2, 2)), dma((8, 2)),
            dma((2, 2)), dma((4,)), dma((8,)), dma((8,)),
            dma((4, 4, 2)), dma((16, 2)),
            dma((2, 16)), dma((2, 16)), dma((2, 16)), dma((2, 16)), dma((4,)), dma((4,)),
        ],
        compiler_params=pltpu.CompilerParams(
            collective_id=0, has_side_effects=True, vmem_limit_bytes=60 * 1024 * 1024
        ),
    )(
        tokens, query_weight, key_weight, value_weight, gate_weight,
        forget_weight.T, forget_bias.reshape(1, 16), out_weight,
    )


def solution(mesh):
    placed = (
        P(("sp", "tp"), None), P(None, "tp"), P(None, "tp"), P(None, "tp"), P(None, "tp"), P(), P(), P(),
    )
    return jax.shard_map(
        body, mesh=mesh, in_specs=placed, out_specs=P(("sp", "tp"), None), check_vma=False
    )
```

```python
import jax
import jax.numpy as jnp
from jax import lax
from jax.experimental import pallas as pl
from jax.experimental.pallas import tpu as pltpu
from jax.sharding import PartitionSpec as P

NZ, NX, NY = 8, 4, 4
HD = 128
WIDTH = 256
D = 2048
SUB = 128
ROW = 64
HALF = 32
PARTS = (
    ((0, 0, ROW, 0),),
    ((NY - 1, 0, HALF, 0), (1, HALF, HALF, HALF)),
    ((NY - 1, 0, HALF, HALF), (1, HALF, HALF, 0)),
    ((2, 0, ROW, 0),),
)
MESH = pl.DeviceIdType.MESH
NT = (((1,), (1,)), ((), ()))
F32, BF16 = jnp.float32, jnp.bfloat16
LOG2E = 1.4426950408889634


def rcopy(src, dst, send, recv, sp, tp):
    return pltpu.make_async_remote_copy(
        src_ref=src,
        dst_ref=dst,
        send_sem=send,
        recv_sem=recv,
        device_id=(sp, tp),
        device_id_type=MESH,
    )


def kernel(
    tok_hbm, wq_hbm, wk_hbm, wv_hbm, wg_hbm, fw_hbm, fb_hbm, wo_hbm, out_ref,
    tok, wq, wk, wv, wg, fw_ref, fb_ref, wo, kvs, qs, gbuf, ggot, lg, lcs, lcbuf, cu, kv, q, acc, mx, ln, ob, obuf, att, fout,
    loc_s, ty_s, ty_r, tr_s, tr_r, tp_s, tp_r,
    xk_s, xk_r, xq_s, xq_r, g_s, g_r, l_s, l_r, lz_s, lz_r, o_s, o_r,
    zs, zr, ps, pr, po_s, po_r,
):
    sp = lax.axis_index("sp")
    tp = lax.axis_index("tp")
    z, x = sp // NX, sp % NX
    y, c = tp // 2, tp % 2
    other = y * 2 + (1 - c)
    up = ((z + 1) % NZ) * NX + x
    down = ((z + NZ - 1) % NZ) * NX + x
    ynext = ((y + 1) % NY) * 2 + c
    yprev = ((y + NY - 1) % NY) * 2 + c
    mine = pl.ds(pl.multiple_of(c * ROW, ROW), ROW)

    barrier = pltpu.get_barrier_semaphore()

    def greet(who_sp, who_tp):
        pl.semaphore_signal(barrier, inc=1, device_id=(who_sp, who_tp), device_id_type=MESH)

    greet(sp, other)
    for dy in range(1, NY):
        for core in range(2):
            greet(sp, ((y + dy) % NY) * 2 + core)
    for dz in (1, 2, NZ - 1, NZ - 2):
        greet(((z + dz) % NZ) * NX + x, tp)
    for dx in range(1, NX):
        for core in range(2):
            greet(z * NX + (x + dx) % NX, y * 2 + core)

    tok_cp = pltpu.make_async_copy(tok_hbm, tok.at[0, mine], loc_s.at[0])
    tok_cp.start()
    loads = [
        pltpu.make_async_copy(src, dst, loc_s.at[1 + n])
        for n, (src, dst) in enumerate(
            ((wk_hbm, wk), (wv_hbm, wv), (wq_hbm, wq), (wg_hbm, wg), (fw_hbm, fw_ref), (fb_hbm, fb_ref), (wo_hbm, wo))
        )
    ]
    for cp in loads[:6]:
        cp.start()

    tok_cp.wait()
    pl.semaphore_wait(barrier, 2 * NY - 1 + 4 + (NX - 1) * 2)

    def rows32(first):
        return pl.ds(pl.multiple_of(c * ROW + first, HALF), HALF)

    def tok_up(h):
        return rcopy(
            tok.at[0, rows32(h * HALF)], tok.at[1 + h, rows32(0)], ty_s.at[0, h], ty_r.at[0, h], sp, ynext
        )

    def tok_down(h):
        return rcopy(
            tok.at[0, rows32(h * HALF)], tok.at[2 - h, rows32(HALF)], ty_s.at[1, h], ty_r.at[1, h], sp, yprev
        )

    def relay_up():
        return rcopy(tok.at[1, rows32(0)], tok.at[3, rows32(0)], tr_s.at[0], tr_r.at[0], sp, ynext)

    def relay_down():
        return rcopy(tok.at[1, rows32(HALF)], tok.at[3, rows32(HALF)], tr_s.at[1], tr_r.at[1], sp, yprev)

    def tok_pair(i):
        return rcopy(tok.at[i, mine], tok.at[i, mine], tp_s.at[i], tp_r.at[i], sp, other)

    def wait_pair(i):
        theirs = pl.ds(pl.multiple_of((1 - c) * ROW, ROW), ROW)
        rcopy(tok.at[i, theirs], tok.at[i, theirs], tp_s.at[i], tp_r.at[i], sp, other).wait_recv()

    tok_up(0).start()
    tok_down(1).start()
    tok_pair(0).start()
    tok_up(1).start()
    tok_down(0).start()

    mx[...] = jnp.full_like(mx, -1e30)
    ln[...] = jnp.zeros_like(ln)
    acc[...] = jnp.zeros_like(acc)

    own_head = x // 2 == c
    own_j = x - 2 * c

    def x_kv(i, j, r):
        rows = pl.ds(r * ROW, ROW)
        return rcopy(
            kvs.at[i, j, :, rows], kv.at[z, i, :, x, rows], xk_s.at[i, j, r], xk_r.at[i, x],
            z * NX + 2 * c + j, y * 2 + r,
        )

    def x_q(i, j, r):
        rows = pl.ds(r * ROW, ROW)
        return rcopy(
            qs.at[i, j, rows], q.at[x, i], xq_s.at[i, j, r], xq_r.at[i, x],
            z * NX + 2 * c + j, y * 2 + r,
        )

    def gate_copy(i, n, cc):
        step, first, rows, into = PARTS[i][n]
        return rcopy(
            gbuf.at[i, pl.ds(cc * ROW + first, rows)], ggot.at[tp, pl.ds(into, rows)],
            g_s.at[i, n, cc], g_r.at[tp, into // HALF], sp, ((y + step) % NY) * 2 + cc,
        )

    def away(j, r):
        return jnp.logical_or(x != 2 * c + j, c != r)

    def project(i):
        part = tok[i]
        k = jnp.dot(part, wk[...], preferred_element_type=F32).astype(BF16)
        v = jnp.dot(part, wv[...], preferred_element_type=F32).astype(BF16)
        for j in range(2):
            kvs[i, j, 0] = k[:, j * HD : (j + 1) * HD]
            kvs[i, j, 1] = v[:, j * HD : (j + 1) * HD]
        for j in range(2):
            for r in range(2):

                @pl.when(away(j, r))
                def _():
                    x_kv(i, j, r).start()

        qq = (jnp.dot(part, wq[...], preferred_element_type=F32) * HD ** (-0.5)).astype(BF16)
        for j in range(2):
            qs[i, j] = qq[:, j * HD : (j + 1) * HD]
        for j in range(2):
            for r in range(2):

                @pl.when(away(j, r))
                def _():
                    x_q(i, j, r).start()

        for j in range(2):

            @pl.when(x == 2 * c + j)
            def _():
                kv[z, i, :, x, mine] = kvs[i, j, :, mine]
                q[x, i] = qs[i, j, mine]

        gate = jax.nn.sigmoid(jnp.dot(part, wg[...], preferred_element_type=F32))
        gbuf[i] = gate
        for cc in range(2):
            if i == 0:

                @pl.when(c != cc)
                def _():
                    gate_copy(i, 0, cc).start()

                @pl.when(c == cc)
                def _():
                    ggot[tp] = gbuf[i, cc * ROW : (cc + 1) * ROW]
            else:
                for n in range(len(PARTS[i])):
                    gate_copy(i, n, cc).start()
        diag = lax.broadcasted_iota(jnp.int32, (16, 16), 0) == lax.broadcasted_iota(jnp.int32, (16, 16), 1)
        bias = jnp.sum(jnp.where(diag, fb_ref[...], 0.0), axis=1, keepdims=True)
        logits = lax.dot_general(fw_ref[...], part, NT, preferred_element_type=F32) + bias
        small = jnp.exp(-jnp.abs(logits))
        grown = 1.0 + small
        tail = jnp.where(grown == 1.0, small, jnp.log(grown) * (small / jnp.where(grown == 1.0, 1.0, grown - 1.0)))
        logs = jnp.minimum(logits, 0.0) - tail
        pick = (
            lax.broadcasted_iota(jnp.int32, (8, 16), 1)
            == lax.broadcasted_iota(jnp.int32, (8, 16), 0) + 2 * tp
        ).astype(F32)
        turned = jnp.dot(pick, logs, precision=lax.Precision.HIGHEST, preferred_element_type=F32)
        lg[i] = turned

    def z_up(o, p, t):
        ref = kv.at[o, p, :, :, mine]
        return rcopy(ref, ref, zs.at[0, t], zr.at[0, t], up, tp)

    def z_down(o, p, t):
        ref = kv.at[o, p, :, :, mine]
        return rcopy(ref, ref, zs.at[1, t], zr.at[1, t], down, tp)

    def z_pair(o, p, way, t):
        ref = kv.at[o, p, :, :, mine]
        return rcopy(ref, ref, ps.at[way, t], pr.at[way, t], sp, other)

    def own_pair(p):
        ref = kv.at[z, p, :, :, mine]
        return rcopy(ref, ref, po_s.at[p], po_r.at[p], sp, other)

    def reach(way, p):
        return 3 + (p < 2).astype(jnp.int32) if way == 0 else 3 + (p >= 2).astype(jnp.int32)

    def goes(way, o, p, d):
        far = reach(way, p)
        if way == 0:
            return jnp.logical_and(d <= far, o + d < NZ)
        return jnp.logical_and(d <= far, o + 1 <= far)

    def first_sends(p):
        for xs in range(NX):

            @pl.when(jnp.logical_not(jnp.logical_and(own_head, x == xs)))
            def _():
                ref = kv.at[z, p, :, xs, mine]
                rcopy(ref, ref, xk_s.at[p, 0, 0], xk_r.at[p, xs], sp, other).wait_recv()

        pv = jnp.int32(p)

        @pl.when(goes(0, z, pv, 1))
        def _():
            z_up(z, p, p).start()

        @pl.when(goes(1, z, pv, 1))
        def _():
            z_down(z, p, p).start()

        own_pair(p).start()

    def origin(way, d):
        return z - d if way == 0 else (z + d) % NZ

    def piece(way, t):
        return t % 4 + (2 * (t >= 12).astype(jnp.int32) if way == 1 else 0)

    def arrives(way, t):
        o = origin(way, t // 4 + 1)
        return jnp.logical_and(o >= 0, goes(way, o, piece(way, t), t // 4 + 1))

    def relay(t):
        d = t // 4 + 1
        for way, hop in ((0, z_up), (1, z_down)):
            o, p = origin(way, d), piece(way, t)

            @pl.when(arrives(way, t))
            def _():
                hop(o, p, t).wait_recv()

                @pl.when(goes(way, o, p, d + 1))
                def _():
                    hop(o, p, t + 4 - (2 * (t >= 8).astype(jnp.int32) if way == 1 else 0)).start()

                @pl.when(o < z)
                def _():
                    z_pair(o, p, way, t).start()

    for cp in loads[:6]:
        cp.wait()
    wait_pair(0)
    project(0)
    loads[6].start()
    tok_up(0).wait_recv()
    relay_up().start()
    tok_down(1).wait_recv()
    relay_down().start()
    tok_pair(1).start()
    first_sends(0)
    wait_pair(1)
    project(1)
    tok_up(1).wait_recv()
    tok_down(0).wait_recv()
    tok_pair(2).start()
    first_sends(1)
    wait_pair(2)
    project(2)
    relay(jnp.int32(0))
    relay_up().wait_recv()
    relay_down().wait_recv()
    tok_pair(3).start()
    first_sends(2)
    relay(jnp.int32(1))
    wait_pair(3)
    project(3)

    even = (lax.broadcasted_iota(jnp.int32, (8, SUB), 1) // HALF) % 2 == 0
    before = jnp.where(even, lg[1], pltpu.roll(lg[2], HALF, 1))
    after = jnp.where(even, pltpu.roll(lg[2], SUB - HALF, 1), lg[1])
    tri = (
        lax.broadcasted_iota(jnp.int32, (SUB, SUB), 0) <= lax.broadcasted_iota(jnp.int32, (SUB, SUB), 1)
    ).astype(F32)
    chips = [lg[0], after, lg[3], before]
    sums = jnp.dot(
        jnp.concatenate(chips, axis=0), tri, precision=lax.Precision.HIGHEST, preferred_element_type=F32
    )
    sums = [sums[n * 8 : (n + 1) * 8] for n in range(NY)]
    totals = [part[:, SUB - 1 : SUB] for part in sums]
    moved = []
    for n in range(NY):
        past = jnp.zeros((8, 1), F32)
        for m in range(NY):
            past = past + jnp.where((y + m) % NY < (y + n) % NY, totals[m], 0.0)
        moved.append(sums[n] + past)
    own, after, far, before = moved
    in_order = (
        own,
        jnp.where(even, before, after),
        jnp.where(even, pltpu.roll(before, SUB - HALF, 1), pltpu.roll(after, HALF, 1)),
        far,
        jnp.broadcast_to((totals[0] + totals[1]) + (totals[2] + totals[3]), (8, SUB)),
    )
    for n, part in enumerate(in_order):
        for j in range(2):
            lcs[j, :, n * SUB : (n + 1) * SUB] = part[j : j + 1]

    def log_copy(j, r):
        return rcopy(lcs.at[j], lcbuf.at[sp], l_s.at[j, r], l_r.at[x], z * NX + 2 * c + j, y * 2 + r)

    for j in range(2):
        for r in range(2):

            @pl.when(away(j, r))
            def _():
                log_copy(j, r).start()

        @pl.when(x == 2 * c + j)
        def _():
            lcbuf[sp] = lcs[j]

    first_sends(3)

    def place(p, row):
        side = (row & HALF) >> 5
        steps = jnp.where(p == 0, 0, jnp.where(p == 3, 2, 3 + 2 * side))
        return ((y + steps) & 3) * SUB + (row ^ jnp.where(p == 2, HALF, 0))

    def attend(pieces, diagonal=False):
        rows = q[...].reshape(NX * 256, HD)
        scores = [
            lax.dot_general(rows, kv[o, p, 0].reshape(NX * SUB, HD), NT, preferred_element_type=F32)
            for o, p in pieces
        ]
        biases = [cu[o, p] for o, p in pieces]
        rounded, factors = [], []
        for b in range(NX):
            parts = []
            for score, bias in zip(scores, biases):
                s = score[b * 256 : (b + 1) * 256] * LOG2E - bias
                if diagonal:
                    row = lax.broadcasted_iota(jnp.int32, (256, 1), 0)
                    at_q = b * 512 + place(row >> 6, c * ROW + (row & 63))
                    lane = lax.broadcasted_iota(jnp.int32, (1, NX * SUB), 1)
                    at_k = (lane >> 7) * 512 + place(pieces[0][1], lane & 127)
                    s = jnp.where(at_k <= at_q, s, -jnp.inf)
                parts.append(s)
            old = mx[b]
            new = old
            for s in parts:
                new = jnp.maximum(new, jnp.max(s, axis=1, keepdims=True))
            factor = jnp.exp2(old - new)
            weights = [jnp.exp2(s[:, n * 128 : (n + 1) * 128] - new) for s in parts for n in range(NX)]
            sums = weights
            while len(sums) > 1:
                sums = [sums[n] + sums[n + 1] for n in range(0, len(sums), 2)]
            ln[b] = ln[b] * factor + sums[0]
            rounded.append(jnp.concatenate([w.astype(BF16) for w in weights], axis=1))
            factors.append(factor)
            mx[b] = new
        values = [kv[o, p, 1].reshape(NX * SUB, HD) for o, p in pieces]
        values = values[0] if len(values) == 1 else jnp.concatenate(values, axis=0)
        more = jnp.dot(jnp.concatenate(rounded, axis=0), values, preferred_element_type=F32)
        for b in range(NX):
            acc[b] = acc[b] * factors[b] + more[b * 256 : (b + 1) * 256]

    for xs in range(NX):

        @pl.when(jnp.logical_not(jnp.logical_and(own_head, x == xs)))
        def _():
            ref = lcbuf.at[z * NX + xs]
            rcopy(ref, ref, l_s.at[0, 0], l_r.at[xs], sp, other).wait_recv()

    HOPS = ((0, 1), (0, 2), (0, NZ - 1), (0, NZ - 2), (NZ - 1, 2), (NZ - 2, 2), (1, NZ - 2))

    def z_logs(n):
        whose, dz = HOPS[n]
        block = (z + whose) % NZ
        ref = lcbuf.at[pl.ds(block * NX, NX)]
        return rcopy(ref, ref, lz_s.at[n], lz_r.at[block], ((z + dz) % NZ) * NX + x, tp)

    def z_logs_wait(back):
        block = (z + NZ - back) % NZ
        ref = lcbuf.at[pl.ds(block * NX, NX)]
        rcopy(ref, ref, lz_s.at[0], lz_r.at[block], sp, other).wait_recv()

    for n in range(4):
        z_logs(n).start()

    offset = jnp.zeros((1, 1), F32)
    for n in range(NX):
        line = lcbuf[z * NX + n]
        scaled = (line + offset) * LOG2E
        for i in range(NY):
            cu[z, i, :, n * SUB : (n + 1) * SUB] = scaled[:, i * SUB : (i + 1) * SUB]
        offset = offset + line[:, 512:513]

    for i in range(NY):
        for xs in range(NX):

            @pl.when(jnp.logical_not(jnp.logical_and(own_head, x == xs)))
            def _():
                ref = q.at[xs, i]
                rcopy(ref, ref, xq_s.at[i, 0, 0], xq_r.at[i, xs], sp, other).wait_recv()

    theirs = pl.ds(pl.multiple_of((1 - c) * ROW, ROW), ROW)

    def pair_wait(o, p, sem):
        ref = kv.at[o, p, :, :, theirs]
        rcopy(ref, ref, po_s.at[0], sem, sp, other).wait_recv()

    def consume(t):
        d = t // 4 + 1
        ups = arrives(0, t)
        o_up, o_down = origin(0, d), origin(1, d)
        p_up, p_down = piece(0, t), piece(1, t)
        downs = jnp.logical_and(arrives(1, t), o_down < z)

        @pl.when(ups)
        def _():
            pair_wait(o_up, p_up, pr.at[0, t])

        @pl.when(downs)
        def _():
            pair_wait(o_down, p_down, pr.at[1, t])

        @pl.when(jnp.logical_and(ups, downs))
        def _():
            attend([(o_up, p_up), (o_down, p_down)])

        @pl.when(jnp.logical_xor(ups, downs))
        def _():
            attend([(jnp.where(ups, o_up, o_down), jnp.where(ups, p_up, p_down))])

    def own_piece(t, carry):
        @pl.when(t == 2)
        def _():
            relay(t + 1)

        pair_wait(z, t, po_r.at[t])
        attend([(z, t)], diagonal=True)
        return carry

    relay(jnp.int32(2))
    lax.fori_loop(0, 2, own_piece, 0)
    for back in (1, 2, NZ - 1):
        z_logs_wait(back)
    for n in range(4, 7):
        z_logs(n).start()
    lax.fori_loop(2, 4, own_piece, 0)
    for back in (3, 4, 5, 6):
        z_logs_wait(back)

    base = jnp.zeros((1, 1), F32)
    for n in range(NZ * NX):
        base = base + jnp.where(n < NX * z, lcbuf[n, :, 512:513], 0.0)
    offset = -base
    for n in range(NZ * NX):
        line = lcbuf[n]
        scaled = (line + offset) * LOG2E
        for i in range(NY):
            cu[n // NX, i, :, (n % NX) * SUB : (n % NX + 1) * SUB] = scaled[:, i * SUB : (i + 1) * SUB]
        offset = offset + line[:, 512:513]

    def step(t, carry):
        @pl.when(jnp.logical_and(t >= 3, t < 13))
        def _():
            relay(t + 1)

        consume(t)
        return carry

    lax.fori_loop(0, 14, step, 0)

    head = y * NX + x

    def out_copy(b, i, n):
        ahead, first, rows, into = PARTS[i][n]
        return rcopy(
            ob.at[b, i, pl.ds(first, rows)], obuf.at[head, pl.ds(into, rows)],
            o_s.at[b, i, n], o_r.at[head, into // HALF], z * NX + b, ((y + ahead) % NY) * 2 + c,
        )

    for b in range(NX):
        done = acc[b] / jnp.sum(ln[b], axis=1, keepdims=True)
        ob[b] = done.astype(BF16).reshape(NY, ROW, HD)
        for i in (3, 1, 2, 0):
            if i == 0:

                @pl.when(x != b)
                def _():
                    out_copy(b, 0, 0).start()

                @pl.when(x == b)
                def _():
                    obuf[head] = ob[b, 0]
            else:
                for n in range(len(PARTS[i])):
                    out_copy(b, i, n).start()

    for h in range(2):
        tok_up(h).wait_send()
        tok_down(h).wait_send()
    relay_up().wait_send()
    relay_down().wait_send()
    for i in range(NY):
        tok_pair(i).wait_send()
        own_pair(i).wait_send()
        for j in range(2):
            for r in range(2):

                @pl.when(away(j, r))
                def _():
                    x_kv(i, j, r).wait_send()
                    x_q(i, j, r).wait_send()

        for cc in range(2):
            for n in range(len(PARTS[i])):

                @pl.when(jnp.logical_or(i != 0, c != cc))
                def _():
                    gate_copy(i, n, cc).wait_send()

    for j in range(2):
        for r in range(2):

            @pl.when(away(j, r))
            def _():
                log_copy(j, r).wait_send()

    for n in range(7):
        z_logs(n).wait_send()

    def drain(t, carry):
        d = t // 4 + 1
        for way, hop in ((0, z_up), (1, z_down)):
            p = piece(way, t)
            src = origin(way, d - 1)

            @pl.when(jnp.logical_and(src >= 0, goes(way, src, p, d)))
            def _():
                hop(src, p, t).wait_send()

            o = origin(way, d)

            @pl.when(jnp.logical_and(arrives(way, t), o < z))
            def _():
                z_pair(o, p, way, t).wait_send()

        return carry

    lax.fori_loop(0, 14, drain, 0)

    loads[6].wait()
    for ahead in (0, 1, 3, 2):
        yy = (y + ahead) % NY
        for core in range(2):
            who = yy * 2 + core
            for into in range(0, ROW, ROW if ahead % 2 == 0 else HALF):
                ref = ggot.at[who, pl.ds(into, ROW if ahead % 2 == 0 else HALF)]

                def got():
                    rcopy(ref, ref, g_s.at[0, 0, 0], g_r.at[who, into // HALF], sp, other).wait_recv()

                if ahead == 0:
                    pl.when(core != c)(got)
                else:
                    got()
        for xx in range(NX):
            h = yy * NX + xx
            for into in range(0, ROW, ROW if ahead % 2 == 0 else HALF):
                ref = obuf.at[h, pl.ds(into, ROW if ahead % 2 == 0 else HALF)]

                def came():
                    rcopy(ref, ref, o_s.at[0, 0, 0], o_r.at[h, into // HALF], sp, other).wait_recv()

                if ahead == 0:
                    pl.when(xx != x)(came)
                else:
                    came()
            gate = ggot[yy * 2 + xx // 2, :, xx % 2 * HD : (xx % 2 + 1) * HD]
            att[:, xx * HD : (xx + 1) * HD] = (obuf[h].astype(F32) * gate).astype(BF16)
        share = pl.ds(pl.multiple_of(yy * NX * HD, NX * HD), NX * HD)
        for n in range(4):
            cols = slice(n * 512, (n + 1) * 512)
            more = jnp.dot(att[...], wo[share, cols], preferred_element_type=F32)
            if ahead == 0:
                fout[:, cols] = more
            elif ahead != 2:
                fout[:, cols] += more
            else:
                out_ref[:, cols] = (fout[:, cols] + more).astype(BF16)

    for b in range(NX):
        for i in range(NY):
            for n in range(len(PARTS[i])):

                @pl.when(jnp.logical_or(i != 0, x != b))
                def _():
                    out_copy(b, i, n).wait_send()


def body(tokens, query_weight, key_weight, value_weight, gate_weight, forget_weight, forget_bias, out_weight):
    dma = pltpu.SemaphoreType.DMA
    vmem = pltpu.VMEM
    anywhere = pl.BlockSpec(memory_space=pl.ANY)
    local = pl.BlockSpec(memory_space=pltpu.VMEM)
    return pl.pallas_call(
        kernel,
        out_shape=jax.ShapeDtypeStruct((ROW, D), BF16),
        in_specs=[anywhere] * 8,
        out_specs=local,
        scratch_shapes=[
            vmem((NY, SUB, D), BF16),
            vmem((D, WIDTH), BF16),
            vmem((D, WIDTH), BF16),
            vmem((D, WIDTH), BF16),
            vmem((D, WIDTH), BF16),
            vmem((16, D), BF16),
            vmem((1, 16), F32),
            vmem((D, D), BF16),
            vmem((NY, 2, 2, SUB, HD), BF16),
            vmem((NY, 2, SUB, HD), BF16),
            vmem((NY, SUB, WIDTH), F32),
            vmem((8, ROW, WIDTH), F32),
            vmem((NY, 8, SUB), F32),
            vmem((2, 1, 640), F32),
            vmem((NZ * NX, 1, 640), F32),
            vmem((NZ, NY, 1, 512), F32),
            vmem((NZ, NY, 2, NX, SUB, HD), BF16),
            vmem((NX, NY, ROW, HD), BF16),
            vmem((NX, 256, HD), F32),
            vmem((NX, 256, HD), F32),
            vmem((NX, 256, HD), F32),
            vmem((NX, NY, ROW, HD), BF16),
            vmem((16, ROW, HD), BF16),
            vmem((ROW, NX * HD), BF16),
            vmem((ROW, D), F32),
            dma((8,)),
            dma((2, 2)), dma((2, 2)), dma((2,)), dma((2,)), dma((4,)), dma((4,)),
            dma((4, 2, 2)), dma((4, 4)), dma((4, 2, 2)), dma((4, 4)),
            dma((4, 2, 2)), dma((8, 2)),
            dma((2, 2)), dma((4,)), dma((8,)), dma((8,)),
            dma((4, 4, 2)), dma((16, 2)),
            dma((2, 16)), dma((2, 16)), dma((2, 16)), dma((2, 16)), dma((4,)), dma((4,)),
        ],
        compiler_params=pltpu.CompilerParams(
            collective_id=0, has_side_effects=True, vmem_limit_bytes=60 * 1024 * 1024
        ),
    )(
        tokens, query_weight, key_weight, value_weight, gate_weight,
        forget_weight.T, forget_bias.reshape(1, 16), out_weight,
    )


def solution(mesh):
    placed = (
        P(("sp", "tp"), None), P(None, "tp"), P(None, "tp"), P(None, "tp"), P(None, "tp"), P(), P(), P(),
    )
    return jax.shard_map(
        body, mesh=mesh, in_specs=placed, out_specs=P(("sp", "tp"), None), check_vma=False
    )
```
